32 devices in a mesh: ep: 16 (over z, x, core), tp: 2 (over y).
Axes of the slice: x: 2, y: 2, z: 4, core: 2. Of those that a mesh axis runs over, the one named last changes fastest.
Arguments:
- tokens: bfloat16 [256, 2048], P('ep', 'tp'), may hold values from -6 to 6
- state: bfloat16 [256, 32, 4096], P('ep', 'tp'), may hold values from -6 to 6
- mix_gain: float32 [2048], P('tp'), may hold values from 0.1 to 1.9
- w_recept: bfloat16 [2048, 2048], P('tp', 'ep'), may hold values from -0.125 to 0.125
- w_key: bfloat16 [2048, 2048], P('tp', 'ep'), may hold values from -0.125 to 0.125
- w_value: bfloat16 [2048, 2048], P('tp', 'ep'), may hold values from -0.125 to 0.125
- w_decay: bfloat16 [2048, 2048], P('tp', 'ep'), may hold values from -0.125 to 0.125
- w_rate: bfloat16 [2048, 2048], P('tp', 'ep'), may hold values from -0.125 to 0.125
- decay_base: float32 [2048], P('tp'), may hold values from -4 to 2
- rate_base: float32 [2048], P('tp'), may hold values from -2 to 2
- head_gain: float32 [2048], P('tp'), may hold values from 0.1 to 1.9
- w_out: bfloat16 [2048, 2048], P('tp', 'ep'), may hold values from -0.125 to 0.125
- moe_gain: float32 [2048], replicated, may hold values from 0.1 to 1.9
- routes: int32 [256, 6], P('ep'), may hold values from 0 to 15, all different within a row; in each aligned block of 16 rows (0 to 15, 16 to 31, ...) at most 12 rows name the same one
- route_weight: float32 [256, 6], P('ep'), may hold values from 0.1 to 1
- expert_gate: bfloat16 [16, 2048, 512], P('ep', None, 'tp'), may hold values from -0.125 to 0.125
- expert_up: bfloat16 [16, 2048, 512], P('ep', None, 'tp'), may hold values from -0.125 to 0.125
- expert_down: bfloat16 [16, 512, 2048], P('ep', 'tp'), may hold values from -0.25 to 0.25
- shared_gate: bfloat16 [2048, 512], P(None, 'tp'), may hold values from -0.125 to 0.125
- shared_up: bfloat16 [2048, 512], P(None, 'tp'), may hold values from -0.125 to 0.125
- shared_down: bfloat16 [512, 2048], P('tp'), may hold values from -0.25 to 0.25
Outputs:
- layer_out: bfloat16 [256, 2048], P('ep', 'tp')
The draws below stay inside these ranges and needn't reach their ends.
Inputs may be any that keep to these rules, and one draw needn't show every extreme that they name: `routes`: each row names 6 different experts. Within the rows of one device (aligned blocks of 16 rows) no expert is named by more than 12 rows, a bound that some block reaches.
All inputs are finite; a program needn't handle non-finite values.
Results may differ from the reference program's by a relative error of at most 0.024.
Values may be sent and summed in bfloat16 or wider, within the bound.
No kernel may reach another device: no remote copies, remote signals or barrier semaphores. Data moves between devices by JAX's collectives and lax.ppermute only.
A program may use at most 64 MiB of HBM per device.

```python
import math
import jax
import jax.numpy as jnp
import numpy as np
from jax import lax

D = 2048
HEADS = 32
HEAD = 64
F = 512
FS = 512
TOPK = 6
SEQ_DEV = 16
TOKENS = 256
EXPERTS = 16
CAP = 12
DA = 2048
N_EP = 16
N_TP = 2


def shard_levels(stream_key, shape, split, smallest, top_value):
    gain, own = 1.0, jax.random.fold_in(stream_key, 6)
    for dim, parts in split:
        heights = jnp.exp(jax.random.uniform(jax.random.fold_in(own, dim), (parts,), jnp.float32, smallest / len(split), top_value / len(split)))
        gain = gain * jnp.repeat(heights, shape[dim] // parts).reshape([-1 if axis == dim else 1 for axis in range(len(shape))])
    return gain


def deal_out(own_key, own, number, rows, number_of, top, bound, slope):
    ranking = jax.random.permutation(own_key, number_of)
    packed, usual = portions_of(number_of, rows * top, bound, slope, True), portions_of(number_of, rows * top, bound, slope, False)
    places = jnp.arange(number_of)

    def named(lengths, offset_by):
        used = int((lengths > 0).sum())
        fixed = max(1, used // 4)
        shifted = fixed + (places - fixed + offset_by * (used - fixed)) % max(1, number_of - fixed)
        return jnp.zeros((number_of,), jnp.int32).at[ranking[jnp.where(places < fixed, places, shifted)]].set(jnp.asarray(lengths, jnp.int32))

    lengths = jnp.where(number % 4 == 0, named(packed, number // 4), named(usual, number - number // 4 - 1))
    mixed = jax.random.permutation(jax.random.fold_in(own, 3), number_of)
    giver, sink = mixed[0:number_of // 2 * 2:2], mixed[1:number_of // 2 * 2:2]
    slack = jnp.minimum(lengths[giver] - 1, bound - lengths[sink]) // 2
    slack = jnp.where((giver == ranking[0]) | (sink == ranking[0]) | (lengths[sink] == 0), 0, jnp.maximum(slack, 0))
    shifted = jax.random.randint(jax.random.fold_in(own, 4), (number_of // 2,), 0, 1 << 20) % (slack + 1)
    lengths = lengths.at[giver].add(-shifted).at[sink].add(shifted)
    items = jnp.searchsorted(jnp.cumsum(lengths), jnp.arange(rows * top), side="right").astype(jnp.int32)
    table = items.reshape(top, rows).T
    table = table[jax.random.permutation(jax.random.fold_in(own, 1), rows)]
    offset_by = jax.random.randint(jax.random.fold_in(own, 2), (rows, 1), 0, top)
    return jnp.take_along_axis(table, (jnp.arange(top)[None, :] + offset_by) % top, axis=1)


def portions_of(count, total, most, lean, full):
    portions = [(1 << 20) // math.isqrt(grade ** lean) + 1 for grade in range(1, count + 1)]
    largest = most if full else min(most, max(-(-total // count), total * portions[0] // sum(portions)))
    least = 1 if total - largest >= count - 1 else 0
    counts, surplus = [largest] + [least] * (count - 1), total - largest - least * (count - 1)
    while surplus > 0:
        candidates = [i for i in range(1, count) if counts[i] < largest] or [i for i in range(1, count) if counts[i] < most]
        mass, left = sum([portions[i] for i in candidates]), surplus
        for i in candidates:
            more = min(most - counts[i], max(1, left * portions[i] // mass), surplus)
            counts[i] = counts[i] + more
            surplus = surplus - more
    return np.array(counts)


def gaussian(rng, shape, width, bound, shards=(), kind=jnp.bfloat16):
    drawn = width * jax.random.normal(rng, shape, jnp.float32)
    if shards:
        drawn = drawn * shard_levels(rng, shape, shards, -0.22, 0.18)
    return jnp.clip(drawn, -bound, bound).astype(kind)


def setup_inputs(seed: int = 0) -> dict:
    splits = jax.random.split(jax.random.key(seed), 22)
    tokens = gaussian(splits[0], (TOKENS, D), 1.0, 6.0, ((0, 16), (1, 2)))
    state = gaussian(splits[1], (TOKENS, HEADS, HEAD * HEAD), 1.0, 6.0, ((0, 16), (1, 2)))
    mix_gain = jnp.clip(1.0 + 0.18 * jax.random.normal(splits[2], (D,), jnp.float32), 0.1, 1.9)
    w_recept = gaussian(splits[3], (D, DA), D ** -0.5, 0.125, ((0, 2), (1, 16)))
    w_key = gaussian(splits[4], (D, DA), D ** -0.5, 0.125, ((0, 2), (1, 16)))
    w_value = gaussian(splits[5], (D, DA), D ** -0.5, 0.125, ((0, 2), (1, 16)))
    w_decay = gaussian(splits[6], (D, DA), D ** -0.5, 0.125, ((0, 2), (1, 16)))
    w_rate = gaussian(splits[7], (D, DA), D ** -0.5, 0.125, ((0, 2), (1, 16)))
    decay_base = jnp.clip(-4.0 + 6.0 * jax.random.uniform(splits[8], (DA,), jnp.float32) ** shard_levels(splits[8], (DA,), ((0, 2),), -0.2, 0.2), -4.0, 2.0)
    rate_base = jnp.clip(jax.random.uniform(splits[9], (DA,), jnp.float32, -2.0, 2.0) * shard_levels(splits[9], (DA,), ((0, 2),), -0.4, 0.0), -2.0, 2.0)
    head_gain = jnp.clip(1.0 + 0.18 * jax.random.normal(splits[10], (DA,), jnp.float32), 0.1, 1.9)
    w_out = gaussian(splits[11], (DA, D), DA ** -0.5, 0.125, ((0, 2), (1, 16)))
    moe_gain = jnp.clip(1.0 + 0.18 * jax.random.normal(splits[12], (D,), jnp.float32), 0.1, 1.9)
    routes_keys = jax.random.split(jax.random.fold_in(splits[13], 1), TOKENS // SEQ_DEV)
    routes_turns = jax.random.permutation(jax.random.fold_in(splits[13], 3), TOKENS // SEQ_DEV)
    routes = jax.vmap(lambda own, number: deal_out(jax.random.fold_in(splits[13], 2), own, number, SEQ_DEV, EXPERTS, TOPK, CAP, 2))(routes_keys, routes_turns).reshape((TOKENS, TOPK))
    route_weight = jnp.clip(jnp.exp(math.log(1.0) - 2.3025851 * jax.random.uniform(splits[14], (TOKENS, TOPK), jnp.float32) ** shard_levels(splits[14], (TOKENS, TOPK), ((0, 16),), -0.2, 0.2)), 0.1, 1.0)
    expert_gate = gaussian(splits[15], (EXPERTS, D, F), D ** -0.5, 0.125, ((0, 16), (2, 2)))
    expert_up = gaussian(splits[16], (EXPERTS, D, F), D ** -0.5, 0.125, ((0, 16), (2, 2)))
    expert_down = gaussian(splits[17], (EXPERTS, F, D), F ** -0.5, 0.25, ((0, 16), (1, 2)))
    shared_gate = gaussian(splits[18], (D, FS), D ** -0.5, 0.125, ((1, 2),))
    shared_up = gaussian(splits[19], (D, FS), D ** -0.5, 0.125, ((1, 2),))
    shared_down = gaussian(splits[20], (FS, D), FS ** -0.5, 0.25, ((0, 2),))
    return dict(tokens=tokens, state=state, mix_gain=mix_gain, w_recept=w_recept, w_key=w_key, w_value=w_value, w_decay=w_decay, w_rate=w_rate, decay_base=decay_base, rate_base=rate_base, head_gain=head_gain, w_out=w_out, moe_gain=moe_gain, routes=routes, route_weight=route_weight, expert_gate=expert_gate, expert_up=expert_up, expert_down=expert_down, shared_gate=shared_gate, shared_up=shared_up, shared_down=shared_down)


RMS_EPS = 1e-06
GN_EPS = 0.00064
KEY_EPS = 1e-06
ROUTED_SCALE = 2.5

def row_norm(row_vals, gain_vals):
    row32 = row_vals.astype(jnp.float32)
    factor = lax.rsqrt(lax.optimization_barrier(jnp.mean(row32 * row32, axis=-1, keepdims=True)) + RMS_EPS)
    return (row32 * factor * gain_vals).astype(jnp.bfloat16)

def quarter_dot(left_vals, weight):
    row_count = left_vals.shape[0]
    part_len = left_vals.shape[1] // N_TP
    left_parts = left_vals.reshape(row_count, N_TP, part_len).astype(jnp.float32)
    weight_parts = weight.reshape(N_TP, part_len, weight.shape[1]).astype(jnp.float32)
    partial_value = jnp.einsum('rqk,qkm->rqm', left_parts, weight_parts)
    rounded = lax.optimization_barrier(partial_value.astype(jnp.bfloat16))
    return lax.optimization_barrier(jnp.sum(rounded.astype(jnp.float32), axis=1))

def mixer_rows(state_rows, projected, decay_base, rate_base, head_gain):
    seq_count = projected.shape[0]
    head_count = projected.shape[2] // HEAD

    def per_head(column):
        return projected[:, column, :].reshape(seq_count, head_count, HEAD)
    receptance = per_head(0)
    key_vec = per_head(1)
    value_vec = per_head(2)
    decay_pre = (projected[:, 3, :] + decay_base).reshape(seq_count, head_count, HEAD)
    rate_pre = (projected[:, 4, :] + rate_base).reshape(seq_count, head_count, HEAD)
    decay_rate = jnp.exp(-jnp.exp(-jax.nn.softplus(-decay_pre) - 0.5))
    in_rate = jax.nn.sigmoid(rate_pre)
    unit_key = key_vec * lax.rsqrt(lax.optimization_barrier(jnp.sum(key_vec * key_vec, axis=-1, keepdims=True)) + KEY_EPS)
    carried = state_rows.astype(jnp.float32).reshape(seq_count, head_count, HEAD, HEAD)
    removed = jnp.einsum('nhvk,nhk->nhv', carried, unit_key)
    updated = carried * decay_rate[:, :, None, :] - removed[:, :, :, None] * (unit_key * in_rate)[:, :, None, :] + value_vec[:, :, :, None] * (key_vec * in_rate)[:, :, None, :]
    readout = jnp.einsum('nhvk,nhk->nhv', updated, receptance)
    centre = lax.optimization_barrier(jnp.mean(readout, axis=-1, keepdims=True))
    spread = lax.optimization_barrier(jnp.mean(jnp.square(readout - centre), axis=-1, keepdims=True))
    normed = (readout - centre) * lax.rsqrt(spread + GN_EPS)
    return (normed.reshape(seq_count, head_count * HEAD) * head_gain).astype(jnp.bfloat16)

def reference(tokens, state, mix_gain, w_recept, w_key, w_value, w_decay, w_rate, decay_base, rate_base, head_gain, w_out, moe_gain, routes, route_weight, expert_gate, expert_up, expert_down, shared_gate, shared_up, shared_down):
    normed = row_norm(tokens, mix_gain)
    projected = jnp.stack([quarter_dot(normed, weight) for weight in (w_recept, w_key, w_value, w_decay, w_rate)], axis=1)

    def mix_group(item):
        return mixer_rows(item[0], item[1], decay_base, rate_base, head_gain)
    mixed = lax.map(mix_group, (state.reshape(N_EP, SEQ_DEV, HEADS, HEAD * HEAD), projected.reshape(N_EP, SEQ_DEV, 5, HEADS * HEAD)))
    mixed = mixed.reshape(TOKENS, HEADS * HEAD)
    attended = quarter_dot(mixed, w_out)
    resid = (tokens.astype(jnp.float32) + attended).astype(jnp.bfloat16)
    normed_two = row_norm(resid, moe_gain)
    shared_hidden = (jax.nn.silu(jnp.dot(normed_two, shared_gate, preferred_element_type=jnp.float32)) * jnp.dot(normed_two, shared_up, preferred_element_type=jnp.float32)).astype(jnp.bfloat16)
    shared_out = quarter_dot(shared_hidden, shared_down)
    per_group = SEQ_DEV * TOPK
    grouped = routes.reshape(N_EP, per_group)
    position = jnp.arange(per_group, dtype=jnp.int32)
    earlier = (grouped[:, :, None] == grouped[:, None, :]) & (position[None, None, :] < position[None, :, None])
    rank_in = lax.optimization_barrier(jnp.sum(earlier.astype(jnp.int32), axis=2))
    group_ids = jnp.arange(N_EP, dtype=jnp.int32)[:, None]
    flat_slot = ((grouped * N_EP + group_ids) * CAP + rank_in).reshape(-1).astype(jnp.int32)
    owner_token = (jnp.arange(TOKENS, dtype=jnp.int32)[:, None] + jnp.zeros((1, TOPK), jnp.int32)).reshape(-1)
    slot_total = EXPERTS * N_EP * CAP
    table = jnp.zeros((slot_total,), jnp.int32).at[flat_slot].set(owner_token)
    live = jnp.zeros((slot_total,), jnp.float32).at[flat_slot].set(1.0)

    def run_expert(item):
        row_index, live_rows, gate_w, up_w, down_w = item
        chosen_rows = jnp.take(normed_two, row_index, axis=0)
        gate_val = jnp.dot(chosen_rows, gate_w, preferred_element_type=jnp.float32)
        up_val = jnp.dot(chosen_rows, up_w, preferred_element_type=jnp.float32)
        hidden = (jax.nn.silu(gate_val) * up_val).astype(jnp.bfloat16)
        return (quarter_dot(hidden, down_w) * live_rows[:, None]).astype(jnp.bfloat16)
    expert_rows = lax.map(run_expert, (table.reshape(EXPERTS, N_EP * CAP), live.reshape(EXPERTS, N_EP * CAP), expert_gate, expert_up, expert_down))
    picked = jnp.take(expert_rows.reshape(slot_total, D), flat_slot, axis=0)
    picked = picked.astype(jnp.float32).reshape(TOKENS, TOPK, D)
    share = route_weight / lax.optimization_barrier(jnp.sum(route_weight, axis=1, keepdims=True)) * ROUTED_SCALE
    routed = lax.optimization_barrier(jnp.sum(share[:, :, None] * picked, axis=1))
    return (resid.astype(jnp.float32) + routed + shared_out).astype(jnp.bfloat16)
```

```python
import jax
import jax.numpy as jnp
from jax import lax
from jax.sharding import Mesh, PartitionSpec as P

HEAD = 64


RMS_EPS = 1e-06
GN_EPS = 0.00064
KEY_EPS = 1e-06
ROUTED_SCALE = 2.5

F32 = jnp.float32
BF16 = jnp.bfloat16


def core_swap(array):
    return lax.ppermute(array, "core", [(0, 1), (1, 0)])


def spread_rows(rows):
    chips = lax.axis_size("chip")
    copies = jnp.broadcast_to(rows[None], (chips,) + rows.shape)
    return lax.all_to_all(copies, "chip", 0, 0, tiled=True)


def both(own, other):
    core = lax.axis_index("core")
    first = jnp.where(core == 0, own, other)
    second = jnp.where(core == 0, other, own)
    return first, second


def body(
    tokens,
    state,
    mix_gain,
    w_recept,
    w_key,
    w_value,
    w_decay,
    w_rate,
    decay_base,
    rate_base,
    head_gain,
    w_out,
    moe_gain,
    routes,
    route_weight,
    expert_gate,
    expert_up,
    expert_down,
    shared_gate,
    shared_up,
    shared_down,
):
    chips = lax.axis_size("chip")
    tp = lax.axis_size("tp")
    chip = lax.axis_index("chip")
    core = lax.axis_index("core")
    shard = lax.axis_index("tp")
    seqs, part = tokens.shape
    width = part * tp
    cols = w_out.shape[1]
    wide = 2 * cols
    experts = 2 * chips
    topk = routes.shape[1]
    chips_tp = chips // tp

    weights = (w_recept, w_key, w_value, w_decay, w_rate)
    roles = len(weights)
    own_w = jnp.concatenate(weights, axis=1)
    other_w = core_swap(own_w)
    other_out = core_swap(w_out)
    other_gate = core_swap(expert_gate[0])
    other_up = core_swap(expert_up[0])
    other_down = core_swap(expert_down[0])

    rows = spread_rows(tokens).reshape(chips * seqs, part)
    scaled = (rows.astype(F32) * mix_gain).astype(BF16)
    own_p = jnp.dot(scaled, own_w, preferred_element_type=F32).astype(BF16)
    other_p = jnp.dot(scaled, other_w, preferred_element_type=F32).astype(BF16)
    first, second = both(own_p, other_p)
    first = first.reshape(chips, seqs, roles, cols)
    second = second.reshape(chips, seqs, roles, cols)
    sent = jnp.concatenate((first, second), axis=3)
    got = lax.all_to_all(sent, "chip", 0, 0, tiled=True).reshape(
        tp, chips_tp, seqs, roles, wide
    )
    square_sum = jnp.sum(jnp.square(tokens.astype(F32)), axis=1)
    square_tile = jnp.broadcast_to(square_sum[:, None], (seqs, 128))
    total = lax.dynamic_index_in_dim(got, shard, 0, keepdims=False).astype(F32)
    square_total = square_tile
    for step in range(1, tp):
        order = [(i, (i + step) % tp) for i in range(tp)]
        block = lax.dynamic_index_in_dim(got, (shard + step) % tp, 0, keepdims=False)
        total = total + lax.ppermute(block, "tp", order).astype(F32)
        square_total = square_total + lax.ppermute(square_tile, "tp", order)
    factor = lax.rsqrt(square_total[:, :1] / width + RMS_EPS)
    projected = total.transpose(2, 1, 0, 3).reshape(roles, seqs, chips_tp * wide) * factor[None]

    heads = part // HEAD

    def per_head(flat):
        return flat.reshape(seqs, heads, HEAD)

    receptance, key_vec, value_vec = (per_head(projected[i]) for i in range(3))
    decay_pre = per_head(projected[3] + decay_base)
    in_rate = jax.nn.sigmoid(per_head(projected[4] + rate_base))
    decay_rate = jnp.exp(-jnp.exp(-jax.nn.softplus(-decay_pre) - 0.5))
    unit_key = key_vec * lax.rsqrt(jnp.sum(key_vec * key_vec, axis=-1, keepdims=True) + KEY_EPS)
    carried = state.reshape(seqs, heads, HEAD, HEAD).astype(F32)
    removed = jnp.sum(carried * unit_key[:, :, None, :], axis=-1)
    kept = jnp.sum(carried * (decay_rate * receptance)[:, :, None, :], axis=-1)
    down_by = jnp.sum(unit_key * in_rate * receptance, axis=-1, keepdims=True)
    up_by = jnp.sum(key_vec * in_rate * receptance, axis=-1, keepdims=True)
    readout = kept - removed * down_by + value_vec * up_by
    centre = jnp.mean(readout, axis=-1, keepdims=True)
    spread = jnp.mean(jnp.square(readout - centre), axis=-1, keepdims=True)
    mixed = (readout - centre) * lax.rsqrt(spread + GN_EPS)
    mixed = (mixed.reshape(seqs, part) * head_gain).astype(BF16)

    mixed_rows = spread_rows(mixed).reshape(chips * seqs, part)
    own_o = jnp.dot(mixed_rows, w_out, preferred_element_type=F32)
    other_o = jnp.dot(mixed_rows, other_out, preferred_element_type=F32)
    first, second = both(own_o, other_o)
    partial = jnp.concatenate((first, second), axis=1)
    mine = lax.dynamic_slice_in_dim(rows, (chip % chips_tp) * wide, wide, 1).astype(F32)
    partial = partial + jnp.where(chip // chips_tp == shard, mine, 0.0)
    partial = partial.astype(BF16).reshape(chips, 1, seqs, wide)
    partial = jnp.broadcast_to(partial, (chips, tp, seqs, wide)).reshape(chips * tp, seqs, wide)
    back = lax.all_to_all(partial, ("chip", "tp"), 0, 0, tiled=True)
    resid = jnp.sum(back.reshape(chips, tp, seqs, wide).astype(F32), axis=1)
    resid = resid.transpose(1, 0, 2).reshape(seqs, width).astype(BF16)

    resid32 = resid.astype(F32)
    moe_factor = lax.rsqrt(jnp.mean(resid32 * resid32, axis=1, keepdims=True) + RMS_EPS)
    normed_two = (resid32 * moe_factor * moe_gain).astype(BF16)
    share = route_weight / jnp.sum(route_weight, axis=1, keepdims=True) * ROUTED_SCALE
    hit = routes[:, :, None] == jnp.arange(experts, dtype=jnp.int32)[None, None, :]
    table = jnp.sum(jnp.where(hit, share[:, :, None], 0.0), axis=1)
    table_high = table.astype(BF16)
    table_low = (table - table_high.astype(F32)).astype(BF16)
    tail = -(-2 * experts // 128) * 128
    pad = jnp.zeros((seqs, tail - 2 * experts), BF16)
    packed = jnp.concatenate((normed_two, table_high, table_low, pad), axis=1)
    arrived = spread_rows(packed).reshape(chips * seqs, width + tail)
    expert_in = arrived[:, :width]
    tables = arrived[:, width : width + 2 * experts].astype(F32)
    tables = tables[:, :experts] + tables[:, experts:]
    picks = jnp.arange(experts, dtype=jnp.int32)[None, :]

    def hidden_of(gate, up, expert):
        scale = jnp.sum(jnp.where(picks == expert, tables, 0.0), axis=1, keepdims=True)
        gate_val = jnp.dot(expert_in, gate, preferred_element_type=F32)
        up_val = jnp.dot(expert_in, up, preferred_element_type=F32)
        return (jax.nn.silu(gate_val) * up_val * scale).astype(BF16)

    me = chip * 2 + core
    own_h = hidden_of(expert_gate[0], expert_up[0], me)
    other_h = hidden_of(other_gate, other_up, chip * 2 + 1 - core)
    routed = jnp.dot(own_h, expert_down[0], preferred_element_type=F32)
    routed = routed + jnp.dot(other_h, other_down, preferred_element_type=F32)
    shared_hidden = (
        jax.nn.silu(jnp.dot(normed_two, shared_gate, preferred_element_type=F32))
        * jnp.dot(normed_two, shared_up, preferred_element_type=F32)
    ).astype(BF16)
    shared_part = jnp.dot(shared_hidden, shared_down, preferred_element_type=F32)
    at_home = jnp.arange(chips)[:, None, None] == chip
    routed = routed.reshape(chips, seqs, width) + jnp.where(at_home, shared_part[None], 0.0)
    routed = routed.astype(BF16).reshape(chips, seqs, tp, part).transpose(0, 2, 1, 3)
    routed = routed.reshape(chips * tp, seqs, part)
    returned = lax.all_to_all(routed, ("chip", "tp"), 0, 0, tiled=True)
    added = jnp.sum(returned.astype(F32), axis=0)
    own_resid = lax.dynamic_slice_in_dim(resid, shard * part, part, 1).astype(F32)
    return (own_resid + added).astype(BF16)


def solution(mesh):
    ep, tp = mesh.shape["ep"], mesh.shape["tp"]
    grid = Mesh(mesh.devices.reshape(ep // 2, 2, tp), ("chip", "core", "tp"))
    ep = ("chip", "core")
    placed = (
        P(ep, "tp"),
        P(ep, "tp", None),
        P("tp"),
        P("tp", ep),
        P("tp", ep),
        P("tp", ep),
        P("tp", ep),
        P("tp", ep),
        P("tp"),
        P("tp"),
        P("tp"),
        P("tp", ep),
        P(),
        P(ep, None),
        P(ep, None),
        P(ep, None, "tp"),
        P(ep, None, "tp"),
        P(ep, "tp", None),
        P(None, "tp"),
        P(None, "tp"),
        P("tp", None),
    )
    return jax.shard_map(body, mesh=grid, in_specs=placed, out_specs=P(ep, "tp"), check_vma=False)
```

```python
import functools

import jax
import jax.numpy as jnp
from jax import lax
from jax.experimental import pallas as pl
from jax.experimental.pallas import tpu as pltpu
from jax.sharding import Mesh, PartitionSpec as P

HEAD = 64
LANES = 128


RMS_EPS = 1e-06
GN_EPS = 0.00064
KEY_EPS = 1e-06
ROUTED_SCALE = 2.5

F32 = jnp.float32
BF16 = jnp.bfloat16


def dot(left, right):
    return jnp.dot(left, right, preferred_element_type=F32)


def paired(index, step, count):
    if count & (count - 1) == 0:
        return index ^ step
    return (step - index) % count


def swap_pairs(array, axis, step):
    count = lax.axis_size(axis)
    return lax.ppermute(array, axis, [(i, paired(i, step, count)) for i in range(count)])


def spread_rows(rows):
    copies = jnp.broadcast_to(rows[None], (lax.axis_size("z") * lax.axis_size("x"),) + rows.shape)
    return lax.all_to_all(copies, ("z", "x"), 0, 0, tiled=True)


class Late:
    def __init__(self, source, held, arrival):
        self.held, self.shape = held, held.shape
        self.copy = pltpu.make_async_copy(source, held, arrival)
        self.copy.start()
        self.waited = False

    def __getitem__(self, index):
        if not self.waited:
            self.copy.wait()
            self.waited = True
        return self.held[index]


def call(kernel, outs, place, *operands, scratch=(), late=()):
    hbm, vmem = (pl.BlockSpec(memory_space=space) for space in (pltpu.HBM, pltpu.VMEM))
    leaves, tree = jax.tree.flatten(outs)
    counts = len(operands), len(late), len(leaves), len(scratch)
    operands = [pltpu.with_memory_space_constraint(array, pltpu.VMEM) for array in operands]
    later = [pltpu.with_memory_space_constraint(array, pltpu.HBM) for array in late]
    buffers = [pltpu.VMEM(array.shape, array.dtype) for array in late]
    if late:
        buffers.append(pltpu.SemaphoreType.DMA((len(late),)))

    def with_copies(place, *refs):
        parts = []
        for count in counts:
            parts.append(refs[:count])
            refs = refs[count:]
        given, sources, results, own = parts
        waiting = [
            Late(source, held, refs[-1].at[index])
            for index, (source, held) in enumerate(zip(sources, refs))
        ]
        kernel(place, *given, *waiting, *results, *own)

    return pl.pallas_call(
        with_copies,
        out_shape=jax.tree.unflatten(
            tree, [pltpu.VMEM(leaf.shape, leaf.dtype) for leaf in leaves]
        ),
        in_specs=[pl.BlockSpec(memory_space=pltpu.SMEM)]
        + [vmem] * len(operands)
        + [hbm] * len(later),
        out_specs=jax.tree.map(lambda _: vmem, outs),
        scratch_shapes=list(scratch) + buffers,
        compiler_params=pltpu.CompilerParams(vmem_limit_bytes=24 * 1024 * 1024),
    )(place, *operands, *later)


def fetch_kernel(*refs):
    count = len(refs) // 2
    sources, held, arrivals = refs[:count], refs[count : 2 * count], refs[2 * count]
    copies = [
        pltpu.make_async_copy(source, target, arrivals.at[index])
        for index, (source, target) in enumerate(zip(sources, held))
    ]
    for copy in copies:
        copy.start()
    for copy in copies:
        copy.wait()


def fetch(*arrays):
    return pl.pallas_call(
        fetch_kernel,
        out_shape=[pltpu.VMEM(array.shape, array.dtype) for array in arrays],
        in_specs=[pl.BlockSpec(memory_space=pltpu.HBM)] * len(arrays),
        out_specs=[pl.BlockSpec(memory_space=pltpu.VMEM)] * len(arrays),
        scratch_shapes=[pltpu.SemaphoreType.DMA((len(arrays),))],
        compiler_params=pltpu.CompilerParams(vmem_limit_bytes=24 * 1024 * 1024),
    )(*(pltpu.with_memory_space_constraint(array, pltpu.HBM) for array in arrays))


def square_holder(target, tp, chips_tp):
    return (target + 1) % tp * chips_tp


def project_kernel(sizes, place, rows, gain, *refs):
    tp, chips_tp, roles = sizes
    other, own, out = refs[:roles], refs[roles : 2 * roles], refs[2 * roles]
    core = place[2]
    chips, seqs, part = rows.shape
    cols = own[0].shape[1]
    chip = place[0] * place[4] + place[1]
    group = chip // chips_tp
    count = chips * seqs
    left = rows[...].astype(F32).reshape(count, part)
    square = jnp.sum(left * left, axis=1, keepdims=True)
    high = square.astype(BF16)
    low = (square - high.astype(F32)).astype(BF16)
    scaled = (left * gain[...]).astype(BF16)
    for shift in range(1, tp):
        target = (group + shift) % tp
        for index, vals in enumerate((high, low)):
            vals = jnp.broadcast_to(vals.astype(F32), (count, cols)).astype(BF16)
            out[:, target, 0, index] = vals.reshape(chips, seqs, cols)
    for role in range(roles):
        weight = jnp.concatenate((own[role][...], other[role][...]), axis=1)
        product = dot(scaled, weight).astype(BF16).reshape(chips, seqs, 2 * cols)
        out[:, group, role, core] = product[:, :, :cols]
        out[:, group, role, 1 - core] = product[:, :, cols:]


def project(kernels, place, rows, gain, own, other, tp):
    chips, seqs, part = rows.shape
    cols = own[0].shape[1]
    roles = len(own)
    chips_tp = chips // tp
    shape = (chips, tp, roles, 2, seqs, cols)
    if kernels:
        kernel = functools.partial(project_kernel, (tp, chips_tp, roles))
        out = jax.ShapeDtypeStruct(shape, BF16)
        return call(kernel, out, place, rows, gain, *other, late=own)
    core = place[2]
    group = (place[0] * place[4] + place[1]) // chips_tp
    scaled = (rows.astype(F32) * gain[0]).astype(BF16).reshape(chips * seqs, part)
    pairs = []
    for mine, theirs in zip(own, other):
        sides = jnp.stack((dot(scaled, mine), dot(scaled, theirs))).astype(BF16)
        pairs.append(jnp.where(core == 0, sides, sides[::-1]))
    product = jnp.stack(pairs).reshape(roles, 2, chips, seqs, cols).transpose(2, 0, 1, 3, 4)
    square = jnp.sum(jnp.square(rows.astype(F32)), axis=2)
    high = square.astype(BF16)
    low = (square - high.astype(F32)).astype(BF16)
    marks = jnp.stack((high, low), axis=1)[:, None, :, :, None]
    marks = jnp.broadcast_to(marks, (chips, roles, 2, seqs, cols))
    here = (jnp.arange(tp) == group)[None, :, None, None, None, None]
    return jnp.where(here, product[:, None], marks[:, None])


def gates(decay_pre, rate_pre):
    decay_rate = jnp.exp(-jnp.exp(-jax.nn.softplus(-decay_pre) - 0.5))
    return decay_rate, jax.nn.sigmoid(rate_pre)


def mixer_kernel(place, got, state, decay_base, rate_base, head_gain, out, products, flat):
    chips, tp, _, _, seqs, cols = got.shape
    chips_tp = chips // tp
    heads = state.shape[1]
    count = seqs * heads
    half = count // 2
    shard = place[3]
    holder = square_holder(shard, tp, chips_tp)
    square = jnp.zeros((seqs, cols), F32)
    for source in range(tp):
        for index in range(2):
            square = square + got[holder, source, 0, index].astype(F32)
    factor = lax.rsqrt(square / (heads * HEAD * tp) + RMS_EPS)

    def role(index, base=None):
        vals = jnp.zeros((chips_tp, 2, seqs, cols), F32)
        for source in range(tp):
            vals = vals + got[pl.ds(shard * chips_tp, chips_tp), source, index].astype(F32)
        vals = vals * factor
        if base is not None:
            vals = vals + base[...]
        return vals.reshape(half, LANES)

    receptance, key_vec, value_vec = role(0), role(1), role(2)
    decay_rate, in_rate = gates(role(3, decay_base), role(4, rate_base))
    row = lax.broadcasted_iota(jnp.int32, (LANES, LANES), 0)
    lane = lax.broadcasted_iota(jnp.int32, (LANES, LANES), 1)
    same_head = (row // HEAD == lane // HEAD).astype(F32)

    def head_sum(vals):
        return jnp.dot(
            vals, same_head, precision=lax.Precision.HIGHEST, preferred_element_type=F32
        )

    unit_key = key_vec * lax.rsqrt(head_sum(key_vec * key_vec) + KEY_EPS)
    steer = in_rate * receptance
    down_by = head_sum(unit_key * steer)
    raised = value_vec * head_sum(key_vec * steer)
    side = lax.broadcasted_iota(jnp.int32, (half, LANES), 1) < HEAD
    evens, odds = [], []
    for vals in (decay_rate * receptance, unit_key, raised, down_by):
        turned = pltpu.roll(vals, HEAD, 1)
        evens.append(jnp.where(side, vals, turned))
        odds.append(jnp.where(side, turned, vals))
    stacked = jnp.concatenate(
        (jnp.concatenate(evens, axis=1), jnp.concatenate(odds, axis=1)), axis=0
    )
    high = stacked.astype(BF16)
    low = (stacked - high.astype(F32)).astype(BF16)
    row = lax.broadcasted_iota(jnp.int32, (count, count), 0)
    col = lax.broadcasted_iota(jnp.int32, (count, count), 1)
    block = (col % half) // seqs
    chosen = (row // heads == col % seqs) & (row % heads == 2 * block + col // half)
    chosen = chosen.astype(F32).astype(BF16)
    turned = dot(chosen, high) + dot(chosen, low)
    along, unit, raised, down_by = (
        turned[:, index * LANES : (index + 1) * LANES] for index in range(4)
    )
    along = jnp.concatenate((along, along), axis=1)
    unit = jnp.concatenate((unit, unit), axis=1)
    span = 2 * LANES
    for start in range(0, HEAD * HEAD, span):
        vals = state[:, :, start : start + span].reshape(count, span).astype(F32)
        products[:count, start : start + span] = (vals * along).astype(BF16)
        products[count:, start : start + span] = (vals * unit).astype(BF16)
    row = lax.broadcasted_iota(jnp.int32, (HEAD * HEAD, HEAD), 0)
    col = lax.broadcasted_iota(jnp.int32, (HEAD * HEAD, HEAD), 1)
    sums = dot(products[...], (row // HEAD == col).astype(F32).astype(BF16))
    readout = sums[:count] - sums[count:] * down_by[:, :HEAD] + raised[:, :HEAD]
    readout = readout - jnp.mean(readout, axis=-1, keepdims=True)
    spread = jnp.mean(readout * readout, axis=-1, keepdims=True)
    normed = readout * lax.rsqrt(spread + GN_EPS)
    gain = jnp.broadcast_to(head_gain[...][None], (seqs, heads, HEAD)).reshape(count, HEAD)
    flat[...] = normed * gain
    for index in range(0, heads, 2):
        first = flat[pl.ds(index, seqs, stride=heads), :]
        second = flat[pl.ds(index + 1, seqs, stride=heads), :]
        out[:, index * HEAD : (index + 2) * HEAD] = jnp.concatenate((first, second), axis=1).astype(
            BF16
        )


def mixer(kernels, place, got, state, decay_base, rate_base, head_gain):
    seqs, heads, _ = state.shape
    chips, tp, roles, _, _, cols = got.shape
    chips_tp = chips // tp
    part = heads * HEAD
    if kernels:
        return call(
            mixer_kernel,
            jax.ShapeDtypeStruct((seqs, part), BF16),
            place,
            got,
            state,
            decay_base,
            rate_base,
            head_gain,
            scratch=(
                pltpu.VMEM((2 * seqs * heads, HEAD * HEAD), BF16),
                pltpu.VMEM((seqs * heads, HEAD), F32),
            ),
        )
    shard = place[3]
    holder = square_holder(shard, tp, chips_tp)
    square = lax.dynamic_index_in_dim(got, holder, 0, keepdims=False)[:, 0].astype(F32)
    factor = lax.rsqrt(jnp.sum(square, axis=(0, 1))[:, :1] / (part * tp) + RMS_EPS)
    total = lax.dynamic_slice_in_dim(got, shard * chips_tp, chips_tp, 0)
    total = jnp.sum(total.astype(F32), axis=1) * factor
    total = total.transpose(1, 3, 0, 2, 4).reshape(roles, seqs, part)

    def per_head(vals):
        return vals.reshape(-1, heads, HEAD)

    receptance, key_vec, value_vec = (per_head(total[i]) for i in range(3))
    decay_rate, in_rate = gates(
        per_head(total[3]) + per_head(decay_base), per_head(total[4]) + per_head(rate_base)
    )
    unit_key = key_vec * lax.rsqrt(jnp.sum(key_vec * key_vec, axis=-1, keepdims=True) + KEY_EPS)
    carried = state.reshape(seqs, heads, HEAD, HEAD).astype(F32)
    removed = jnp.sum(carried * unit_key[:, :, None, :], axis=-1)
    kept = jnp.sum(carried * (decay_rate * receptance)[:, :, None, :], axis=-1)
    steer = in_rate * receptance
    down_by = jnp.sum(unit_key * steer, axis=-1, keepdims=True)
    up_by = jnp.sum(key_vec * steer, axis=-1, keepdims=True)
    readout = kept - removed * down_by + value_vec * up_by
    centre = jnp.mean(readout, axis=-1, keepdims=True)
    spread = jnp.mean(jnp.square(readout - centre), axis=-1, keepdims=True)
    mixed = (readout - centre) * lax.rsqrt(spread + GN_EPS)
    return (mixed * head_gain).reshape(seqs, part).astype(BF16)


def attend_kernel(sizes, place, rows, *refs):
    z_size, x_size, tp = sizes
    lines, weights, out = refs[:z_size], refs[-2:-1] + refs[z_size:-2], refs[-1]
    z, x, core, shard = (place[index] for index in range(4))
    seqs, cols = lines[0].shape[0], weights[0].shape[1]
    z_tp = z_size // tp
    left = jnp.concatenate([line[...] for line in lines], axis=0)
    holds = (z // z_tp == shard).astype(F32)
    for step in range(x_size):
        weight = jnp.concatenate([ref[...] for ref in weights[2 * step : 2 * step + 2]], axis=1)
        product = dot(left, weight)
        for side in range(2):
            slot = paired(x, step, x_size) * 2 + (core ^ side)
            offset = pl.multiple_of(((z % z_tp) * 2 * x_size + slot) * cols, cols)
            for line in range(z_size):
                z_to = paired(z, line, z_size)
                token = rows[z_to * x_size + x, :, pl.ds(offset, cols)].astype(F32)
                vals = product[line * seqs : (line + 1) * seqs, side * cols : (side + 1) * cols]
                out[z_to, slot] = (vals + token * holds).astype(BF16)


def attend(kernels, place, rows, lines, weights, tp, x_size):
    z_size = len(lines)
    seqs, part = lines[0].shape
    cols = weights[0].shape[1]
    shape = (z_size, 2 * x_size, seqs, cols)
    if kernels:
        kernel = functools.partial(attend_kernel, (z_size, x_size, tp))
        out = jax.ShapeDtypeStruct(shape, BF16)
        return call(kernel, out, place, rows, *lines, *weights[1:], late=weights[:1])
    z, x, core, shard = (place[index] for index in range(4))
    z_tp = z_size // tp
    z_order = jnp.stack([paired(z, i, z_size) for i in range(z_size)])
    x_order = jnp.stack([paired(x, i // 2, x_size) * 2 + (core ^ (i % 2)) for i in range(2 * x_size)])
    left = jnp.take(jnp.stack(lines), z_order, axis=0).reshape(z_size * seqs, part)
    weight = jnp.take(jnp.stack(weights), jnp.argsort(x_order), axis=0)
    product = jnp.einsum("rk,skc->rsc", left, weight, preferred_element_type=F32)
    token = lax.dynamic_index_in_dim(
        rows.reshape(z_size, x_size, seqs, z_tp, 2 * x_size, cols), x, 1, keepdims=False
    )
    token = lax.dynamic_index_in_dim(token, z % z_tp, 2, keepdims=False).astype(F32)
    product = product.reshape(z_size, seqs, 2 * x_size, cols)
    product = product + jnp.where(z // z_tp == shard, token, 0.0)
    return product.astype(BF16).reshape(z_size, 1, seqs, 2 * x_size * cols)


def residual_kernel(place, tables, *refs):
    *parts, out = refs
    lines, slots, seqs, cols = parts[0].shape
    for line in range(lines):
        for slot in range(slots):
            vals = sum(part[line, slot].astype(F32) for part in parts).astype(BF16)
            for chip in range(out.shape[0]):
                out[chip, line * slots + slot] = vals
    for index in range(tables.shape[0]):
        for chip in range(out.shape[0]):
            out[chip, lines * slots + index] = tables[index]


def residual(kernels, place, parts, tables, chips):
    lines, slots, seqs, cols = parts[0].shape
    tiles = lines * slots + tables.shape[0]
    if kernels:
        shape = jax.ShapeDtypeStruct((chips, tiles, seqs, cols), BF16)
        return call(residual_kernel, shape, place, tables, *parts)
    total = sum(part.astype(F32) for part in parts).astype(BF16)
    total = jnp.concatenate((total.reshape(lines * slots, seqs, cols), tables), axis=0)
    return jnp.broadcast_to(total[None], (chips,) + total.shape)


def expert_kernel(sizes, place, got, gain, *refs):
    x_size, experts = sizes
    own, other, shared = refs[:3], refs[3:6], refs[6:9]
    out, resid, left, home = refs[9:]
    chips, tp, seqs, part = out.shape
    z_size = chips // x_size
    cols = got.shape[3]
    slots = 2 * x_size
    width = part * tp
    count = chips * seqs
    z, x, core, shard = (place[index] for index in range(4))
    chip = z * x_size + x
    for index in range(chips):
        z_to, x_from = divmod(index, x_size)
        square = jnp.zeros((seqs, cols), F32)
        pieces = []
        for z_from in range(z_size):
            for slot in range(slots):
                piece = got[z_from * x_size + x_from, z_to * slots + slot].astype(F32)
                square = square + piece * piece
                pieces.append(piece)
        factor = lax.rsqrt(jnp.sum(square, axis=1, keepdims=True) / width + RMS_EPS)
        for block, piece in enumerate(pieces):
            lanes = slice(block * cols, (block + 1) * cols)
            left[index, :, lanes] = (piece * factor * gain[:, lanes]).astype(BF16)
    for z_part in range(z_size // tp):
        for slot in range(slots):
            block = z_part * slots + slot
            source = (shard * (z_size // tp) + z_part) * x_size + x
            resid[:, block * cols : (block + 1) * cols] = got[source, z * slots + slot]
    rows = left[...].reshape(count, width)
    tables = [
        got[:, z_size * slots + index].astype(F32).reshape(count, cols)
        for index in range(got.shape[1] - z_size * slots)
    ]
    tables = tables[0] if len(tables) == 1 else jnp.concatenate(tables, axis=1)
    lane = lax.broadcasted_iota(jnp.int32, tables.shape, 1)

    def hidden_of(vals, weights):
        gate, up, _ = weights
        return jax.nn.silu(dot(vals, gate[...])) * dot(vals, up[...])

    def scaled(weights, expert):
        hit = (lane == expert) | (lane == experts + expert)
        scale = jnp.sum(jnp.where(hit, tables, 0.0), axis=1, keepdims=True)
        return (hidden_of(rows, weights) * scale).astype(BF16)

    own_hidden = scaled(own, chip * 2 + core)
    other_hidden = scaled(other, chip * 2 + 1 - core)
    home_hidden = hidden_of(left[chip], shared).astype(BF16)
    for target in range(tp):
        for start in range(0, part, 512):
            lanes = slice(start, min(start + 512, part))
            span = slice(target * part + lanes.start, target * part + lanes.stop)
            vals = dot(own_hidden, own[2][:, span]) + dot(other_hidden, other[2][:, span])
            vals = vals.reshape(chips, seqs, lanes.stop - lanes.start)
            home[...] = dot(home_hidden, shared[2][:, span])
            for index in range(chips):
                extra = jnp.where(chip == index, home[...], 0.0)
                out[index, target, :, lanes] = (vals[index] + extra).astype(BF16)


def expert_rows(kernels, place, got, gain, own, other, shared, tp, x_size):
    chips, _, seqs, cols = got.shape
    z_size = chips // x_size
    width = gain.shape[1]
    slots = width // (z_size * cols)
    part = width // tp
    experts = 2 * chips
    if kernels:
        kernel = functools.partial(expert_kernel, (x_size, experts))
        shapes = [
            jax.ShapeDtypeStruct((chips, tp, seqs, part), BF16),
            jax.ShapeDtypeStruct((seqs, part), BF16),
        ]
        scratch = (pltpu.VMEM((chips, seqs, width), BF16), pltpu.VMEM((seqs, 512), F32))
        return call(
            kernel, shapes, place, got, gain, *own, *other, scratch=scratch, late=shared
        )
    chip = place[0] * place[4] + place[1]
    rows = got[:, : z_size * slots].reshape(z_size, x_size, z_size, slots, seqs, cols)
    rows = rows.transpose(2, 1, 4, 0, 3, 5).reshape(chips, seqs, width)
    resid = lax.dynamic_index_in_dim(rows, chip, 0, keepdims=False)
    resid = lax.dynamic_slice_in_dim(resid, place[3] * part, part, 1)
    rows = rows.astype(F32)
    factor = lax.rsqrt(jnp.mean(rows * rows, axis=2, keepdims=True) + RMS_EPS)
    rows = (rows * factor * gain).astype(BF16)
    left = rows.reshape(chips * seqs, width)
    tables = got[:, z_size * slots :].astype(F32).transpose(0, 2, 1, 3).reshape(chips * seqs, -1)
    tables = tables[:, :experts] + tables[:, experts : 2 * experts]
    names = jnp.arange(experts, dtype=jnp.int32)[None, :]

    def hidden_of(vals, weights):
        gate, up, _ = weights
        return jax.nn.silu(dot(vals, gate)) * dot(vals, up)

    def product(weights, expert):
        scale = jnp.sum(jnp.where(names == expert, tables, 0.0), axis=1, keepdims=True)
        return dot((hidden_of(left, weights) * scale).astype(BF16), weights[2])

    routed = product(own, chip * 2 + place[2]) + product(other, chip * 2 + 1 - place[2])
    home = lax.dynamic_index_in_dim(rows, chip, 0, keepdims=False)
    home = dot(hidden_of(home, shared).astype(BF16), shared[2])
    here = jnp.arange(chips)[:, None, None] == chip
    routed = routed.reshape(chips, seqs, width) + jnp.where(here, home[None], 0.0)
    routed = routed.astype(BF16).reshape(chips, seqs, tp, part).transpose(0, 2, 1, 3)
    return routed, resid


def body(
    tokens,
    state,
    mix_gain,
    w_recept,
    w_key,
    w_value,
    w_decay,
    w_rate,
    decay_base,
    rate_base,
    head_gain,
    w_out,
    moe_gain,
    routes,
    route_weight,
    expert_gate,
    expert_up,
    expert_down,
    shared_gate,
    shared_up,
    shared_down,
):
    z_size, x_size, tp = (lax.axis_size(name) for name in ("z", "x", "tp"))
    chips = z_size * x_size
    seqs, part = tokens.shape
    width = part * tp
    cols = w_out.shape[1]
    experts = 2 * chips
    kernels = cols == LANES and seqs == 16 and part % LANES == 0
    z, x, core, shard = (lax.axis_index(name) for name in ("z", "x", "core", "tp"))
    place = (z, x, core, shard, x_size)
    if kernels:
        place = jnp.stack([jnp.int32(index) for index in place])

    rows = spread_rows(tokens)
    own_w = (w_recept, w_key, w_value, w_decay, w_rate)
    other_w = tuple(swap_pairs(weight, "core", 1) for weight in own_w)
    mix_gain = mix_gain.reshape(1, part)
    moe_gain = moe_gain.reshape(1, width)
    blocks = (chips // tp, 2, 1, cols)
    decay_base, rate_base = decay_base.reshape(blocks), rate_base.reshape(blocks)
    head_gain = head_gain.reshape(part // HEAD, HEAD)
    if kernels:
        mix_gain, moe_gain, decay_base, rate_base, head_gain, state = fetch(
            mix_gain, moe_gain, decay_base, rate_base, head_gain, state
        )
    sent = project(kernels, place, rows, mix_gain, own_w, other_w, tp)
    sent = sent.reshape((chips * tp,) + sent.shape[2:])
    got = lax.all_to_all(sent, ("z", "x", "tp"), 0, 0, tiled=True)
    got = got.reshape((chips, tp) + got.shape[1:])
    mixed = mixer(kernels, place, got, state, decay_base, rate_base, head_gain)

    out_w = []
    for step in range(x_size):
        weight = w_out if step == 0 else swap_pairs(w_out, "x", step)
        out_w += [weight, swap_pairs(weight, "core", 1)]
    lines = [mixed] + [swap_pairs(mixed, "z", step) for step in range(1, z_size)]
    partial = attend(kernels, place, rows, lines, out_w, tp, x_size)
    partials = [partial] + [swap_pairs(partial, "tp", step) for step in range(1, tp)]

    share = route_weight / jnp.sum(route_weight, axis=1, keepdims=True) * ROUTED_SCALE
    hit = routes[:, :, None] == jnp.arange(experts, dtype=jnp.int32)[None, None, :]
    table = jnp.sum(jnp.where(hit, share[:, :, None], 0.0), axis=1)
    high = table.astype(BF16)
    low = (table - high.astype(F32)).astype(BF16)
    lanes = partial.shape[3]
    pad = jnp.zeros((seqs, -(2 * experts) % lanes), BF16)
    tables = jnp.concatenate((high, low, pad), axis=1)
    tables = tables.reshape(seqs, -1, lanes).transpose(1, 0, 2)
    packed = residual(kernels, place, partials, tables, chips)
    got = lax.all_to_all(packed, ("z", "x"), 0, 0, tiled=True)

    own = (expert_gate[0], expert_up[0], expert_down[0])
    other = tuple(swap_pairs(weight, "core", 1) for weight in own)
    shared = (shared_gate, shared_up, shared_down)
    routed, resid = expert_rows(
        kernels, place, got, moe_gain, own, other, shared, tp, x_size
    )
    routed = routed.reshape(chips * tp, seqs, part)
    returned = lax.all_to_all(routed, ("z", "x", "tp"), 0, 0, tiled=True)
    return (resid.astype(F32) + jnp.sum(returned.astype(F32), axis=0)).astype(BF16)


def solution(mesh):
    ep, tp = mesh.shape["ep"], mesh.shape["tp"]
    lines = mesh.devices.reshape(ep // 2, 2, tp)
    x_size = len({getattr(device, "coords", (0,))[0] for device in lines[:, 0, 0]})
    grid = Mesh(lines.reshape(-1, x_size, 2, tp), ("z", "x", "core", "tp"))
    ep = ("z", "x", "core")
    placed = (
        P(ep, "tp"),
        P(ep, "tp", None),
        P("tp"),
        P("tp", ep),
        P("tp", ep),
        P("tp", ep),
        P("tp", ep),
        P("tp", ep),
        P("tp"),
        P("tp"),
        P("tp"),
        P("tp", ep),
        P(),
        P(ep, None),
        P(ep, None),
        P(ep, None, "tp"),
        P(ep, None, "tp"),
        P(ep, "tp", None),
        P(None, "tp"),
        P(None, "tp"),
        P("tp", None),
    )
    return jax.shard_map(body, mesh=grid, in_specs=placed, out_specs=P(ep, "tp"), check_vma=False)
```

```python
import functools

import jax
import jax.numpy as jnp
from jax import lax
from jax.experimental import pallas as pl
from jax.experimental.pallas import tpu as pltpu
from jax.sharding import Mesh, PartitionSpec as P

HEAD = 64
LANES = 128


RMS_EPS = 1e-06
GN_EPS = 0.00064
KEY_EPS = 1e-06
ROUTED_SCALE = 2.5

F32 = jnp.float32
BF16 = jnp.bfloat16


def dot(left, right):
    return jnp.dot(left, right, preferred_element_type=F32)


def paired(index, step, count):
    if count & (count - 1) == 0:
        return index ^ step
    return (step - index) % count


def swap_pairs(array, axis, step):
    count = lax.axis_size(axis)
    return lax.ppermute(array, axis, [(i, paired(i, step, count)) for i in range(count)])


def swap_chips(array, step, chips):
    order = [(i, paired(i, step, chips)) for i in range(chips)]
    return lax.ppermute(array, ("z", "x"), order)


def spread_rows(rows):
    copies = jnp.broadcast_to(rows[None], (lax.axis_size("z") * lax.axis_size("x"),) + rows.shape)
    return lax.all_to_all(copies, ("z", "x"), 0, 0, tiled=True)


class Late:
    def __init__(self, source, held, arrival):
        self.held, self.shape = held, held.shape
        self.copy = pltpu.make_async_copy(source, held, arrival)
        self.copy.start()
        self.waited = False

    def __getitem__(self, index):
        if not self.waited:
            self.copy.wait()
            self.waited = True
        return self.held[index]


def call(kernel, outs, place, *operands, scratch=(), late=()):
    hbm, vmem = (pl.BlockSpec(memory_space=space) for space in (pltpu.HBM, pltpu.VMEM))
    leaves, tree = jax.tree.flatten(outs)
    counts = len(operands), len(late), len(leaves), len(scratch)
    operands = [pltpu.with_memory_space_constraint(array, pltpu.VMEM) for array in operands]
    later = [pltpu.with_memory_space_constraint(array, pltpu.HBM) for array in late]
    buffers = [pltpu.VMEM(array.shape, array.dtype) for array in late]
    if late:
        buffers.append(pltpu.SemaphoreType.DMA((len(late),)))

    def with_copies(place, *refs):
        parts = []
        for count in counts:
            parts.append(refs[:count])
            refs = refs[count:]
        given, sources, results, own = parts
        waiting = [
            Late(source, held, refs[-1].at[index])
            for index, (source, held) in enumerate(zip(sources, refs))
        ]
        kernel(place, *given, *waiting, *results, *own)

    return pl.pallas_call(
        with_copies,
        out_shape=jax.tree.unflatten(
            tree, [pltpu.VMEM(leaf.shape, leaf.dtype) for leaf in leaves]
        ),
        in_specs=[pl.BlockSpec(memory_space=pltpu.SMEM)]
        + [vmem] * len(operands)
        + [hbm] * len(later),
        out_specs=jax.tree.map(lambda _: vmem, outs),
        scratch_shapes=list(scratch) + buffers,
        compiler_params=pltpu.CompilerParams(vmem_limit_bytes=24 * 1024 * 1024),
    )(place, *operands, *later)


def fetch_kernel(*refs):
    count = len(refs) // 2
    sources, held, arrivals = refs[:count], refs[count : 2 * count], refs[2 * count]
    copies = [
        pltpu.make_async_copy(source, target, arrivals.at[index])
        for index, (source, target) in enumerate(zip(sources, held))
    ]
    for copy in copies:
        copy.start()
    for copy in copies:
        copy.wait()


def fetch(*arrays):
    return pl.pallas_call(
        fetch_kernel,
        out_shape=[pltpu.VMEM(array.shape, array.dtype) for array in arrays],
        in_specs=[pl.BlockSpec(memory_space=pltpu.HBM)] * len(arrays),
        out_specs=[pl.BlockSpec(memory_space=pltpu.VMEM)] * len(arrays),
        scratch_shapes=[pltpu.SemaphoreType.DMA((len(arrays),))],
        compiler_params=pltpu.CompilerParams(vmem_limit_bytes=24 * 1024 * 1024),
    )(*(pltpu.with_memory_space_constraint(array, pltpu.HBM) for array in arrays))


def project_kernel(place, rows, gain, *refs):
    roles = (len(refs) - 1) // 2
    other, own, out = refs[:roles], refs[roles : 2 * roles], refs[2 * roles]
    core = place[2]
    chips, seqs, part = rows.shape
    cols = own[0].shape[1]
    scaled = (rows[...].astype(F32) * gain[...]).reshape(chips * seqs, part).astype(BF16)
    order = [(role, 1 - core, other[role]) for role in range(roles)]
    order += [(role, core, own[role]) for role in range(roles)]
    for first in range(0, 2 * roles, 2):
        pair = order[first : first + 2]
        weight = jnp.concatenate([ref[...] for _, _, ref in pair], axis=1)
        product = dot(scaled, weight).astype(BF16).reshape(chips, seqs, 2 * cols)
        for index, (role, side, _) in enumerate(pair):
            out[:, role, side] = product[:, :, index * cols : (index + 1) * cols]


def project(kernels, place, rows, gain, own, other):
    chips, seqs, part = rows.shape
    cols = own[0].shape[1]
    roles = len(own)
    if kernels:
        out = jax.ShapeDtypeStruct((chips, roles, 2, seqs, cols), BF16)
        return call(project_kernel, out, place, rows, gain, *other, late=own)
    scaled = (rows.astype(F32) * gain[0]).astype(BF16).reshape(chips * seqs, part)
    pairs = []
    for mine, theirs in zip(own, other):
        sides = jnp.stack((dot(scaled, mine), dot(scaled, theirs))).astype(BF16)
        pairs.append(jnp.where(place[2] == 0, sides, sides[::-1]))
    product = jnp.stack(pairs).reshape(roles, 2, chips, seqs, cols)
    return product.transpose(2, 0, 1, 3, 4)


def square_of(tokens):
    vals = tokens.astype(F32)
    return jnp.sum(vals * vals, axis=1, keepdims=True)


def pick_kernel(place, got, tokens, *outs):
    chips, roles, sides, seqs, cols = got.shape
    chips_tp = chips // (len(outs) + 1)
    count = chips_tp * roles * sides
    square = square_of(tokens[...])
    high = square.astype(BF16).astype(F32)
    for step, out in enumerate(outs):
        target = paired(place[3], step + 1, len(outs) + 1)
        block = got[pl.ds(target * chips_tp, chips_tp)]
        out[:count] = block.reshape(count, seqs, cols)
        out[count] = jnp.broadcast_to(high, (seqs, cols)).astype(BF16)
        out[count + 1] = jnp.broadcast_to(square - high, (seqs, cols)).astype(BF16)


def pick(kernels, place, got, tokens, tp):
    chips, roles, sides, seqs, cols = got.shape
    chips_tp = chips // tp
    count = chips_tp * roles * sides
    if kernels:
        outs = [jax.ShapeDtypeStruct((count + 2, seqs, cols), BF16)] * (tp - 1)
        return call(pick_kernel, outs, place, got, tokens)
    square = square_of(tokens)
    high = square.astype(BF16)
    marks = jnp.stack((high, (square - high.astype(F32)).astype(BF16)))
    marks = jnp.broadcast_to(marks, (2, seqs, cols))
    outs = []
    for step in range(1, tp):
        start = paired(place[3], step, tp) * chips_tp
        block = lax.dynamic_slice_in_dim(got, start, chips_tp, 0)
        outs.append(jnp.concatenate((block.reshape(count, seqs, cols), marks), axis=0))
    return outs


def gates(decay_pre, rate_pre):
    decay_rate = jnp.exp(-jnp.exp(-jax.nn.softplus(-decay_pre) - 0.5))
    return decay_rate, jax.nn.sigmoid(rate_pre)


def mixer_kernel(place, got, tokens, state, *refs):
    *parts, decay_base, rate_base, head_gain, out, products, flat = refs
    chips, roles, sides, seqs, cols = got.shape
    tp = len(parts) + 1
    chips_tp = chips // tp
    heads = state.shape[1]
    count = seqs * heads
    half = count // 2
    blocks = chips_tp * roles * sides
    square = square_of(tokens[...])
    for part in parts:
        square = square + part[blocks].astype(F32) + part[blocks + 1].astype(F32)
    factor = lax.rsqrt(square / (heads * HEAD * tp) + RMS_EPS)
    others = [part[:blocks].reshape(chips_tp, roles, sides, seqs, cols) for part in parts]

    def role(index, base=None):
        vals = got[pl.ds(place[3] * chips_tp, chips_tp), index].astype(F32)
        for other in others:
            vals = vals + other[:, index].astype(F32)
        vals = vals * factor
        if base is not None:
            vals = vals + base[...]
        return vals.reshape(half, LANES)

    receptance, key_vec, value_vec = role(0), role(1), role(2)
    row = lax.broadcasted_iota(jnp.int32, (LANES, LANES), 0)
    lane = lax.broadcasted_iota(jnp.int32, (LANES, LANES), 1)
    same_head = (row // HEAD == lane // HEAD).astype(F32)

    def head_sum(vals):
        return jnp.dot(
            vals, same_head, precision=lax.Precision.HIGHEST, preferred_element_type=F32
        )

    unit_key = key_vec * lax.rsqrt(head_sum(key_vec * key_vec) + KEY_EPS)
    decay_rate, in_rate = gates(role(3, decay_base), role(4, rate_base))
    steer = in_rate * receptance
    down_by = head_sum(unit_key * steer)
    raised = value_vec * head_sum(key_vec * steer)
    side = lax.broadcasted_iota(jnp.int32, (half, LANES), 1) < HEAD
    evens, odds = [], []
    for vals in (decay_rate * receptance, unit_key, raised, down_by):
        turned = pltpu.roll(vals, HEAD, 1)
        evens.append(jnp.where(side, vals, turned))
        odds.append(jnp.where(side, turned, vals))
    stacked = jnp.concatenate(
        (jnp.concatenate(evens, axis=1), jnp.concatenate(odds, axis=1)), axis=0
    )
    high = stacked.astype(BF16)
    low = (stacked - high.astype(F32)).astype(BF16)
    row = lax.broadcasted_iota(jnp.int32, (count, count), 0)
    col = lax.broadcasted_iota(jnp.int32, (count, count), 1)
    block = (col % half) // seqs
    chosen = (row // heads == col % seqs) & (row % heads == 2 * block + col // half)
    chosen = chosen.astype(F32).astype(BF16)
    turned = dot(chosen, high) + dot(chosen, low)
    along, unit, raised, down_by = (
        turned[:, index * LANES : (index + 1) * LANES] for index in range(4)
    )
    along = jnp.concatenate((along, along), axis=1)
    unit = jnp.concatenate((unit, unit), axis=1)
    span = 2 * LANES
    for start in range(0, HEAD * HEAD, span):
        vals = state[:, :, start : start + span].reshape(count, span).astype(F32)
        products[:count, start : start + span] = (vals * along).astype(BF16)
        products[count:, start : start + span] = (vals * unit).astype(BF16)
    row = lax.broadcasted_iota(jnp.int32, (HEAD * HEAD, HEAD), 0)
    col = lax.broadcasted_iota(jnp.int32, (HEAD * HEAD, HEAD), 1)
    sums = dot(products[...], (row // HEAD == col).astype(F32).astype(BF16))
    readout = sums[:count] - sums[count:] * down_by[:, :HEAD] + raised[:, :HEAD]
    readout = readout - jnp.mean(readout, axis=-1, keepdims=True)
    spread = jnp.mean(readout * readout, axis=-1, keepdims=True)
    normed = readout * lax.rsqrt(spread + GN_EPS)
    gain = jnp.broadcast_to(head_gain[...][None], (seqs, heads, HEAD)).reshape(count, HEAD)
    flat[...] = normed * gain
    for index in range(0, heads, 2):
        first = flat[pl.ds(index, seqs, stride=heads), :]
        second = flat[pl.ds(index + 1, seqs, stride=heads), :]
        out[:, index * HEAD : (index + 2) * HEAD] = jnp.concatenate((first, second), axis=1).astype(
            BF16
        )


def mixer(kernels, place, got, tokens, state, parts, decay_base, rate_base, head_gain):
    seqs, heads, _ = state.shape
    chips, roles, sides, _, cols = got.shape
    tp = len(parts) + 1
    chips_tp = chips // tp
    part = heads * HEAD
    if kernels:
        return call(
            mixer_kernel,
            jax.ShapeDtypeStruct((seqs, part), BF16),
            place,
            got,
            tokens,
            state,
            *parts,
            scratch=(
                pltpu.VMEM((2 * seqs * heads, HEAD * HEAD), BF16),
                pltpu.VMEM((seqs * heads, HEAD), F32),
            ),
            late=(decay_base, rate_base, head_gain),
        )
    square = square_of(tokens) + sum(other[-2:].astype(F32).sum(0)[:, :1] for other in parts)
    factor = lax.rsqrt(square / (part * tp) + RMS_EPS)
    total = lax.dynamic_slice_in_dim(got, place[3] * chips_tp, chips_tp, 0).astype(F32)
    for other in parts:
        total = total + other[:-2].astype(F32).reshape(total.shape)
    total = total * factor
    total = total.transpose(1, 3, 0, 2, 4).reshape(roles, seqs, part)

    def per_head(vals):
        return vals.reshape(-1, heads, HEAD)

    receptance, key_vec, value_vec = (per_head(total[i]) for i in range(3))
    decay_rate, in_rate = gates(
        per_head(total[3]) + per_head(decay_base), per_head(total[4]) + per_head(rate_base)
    )
    unit_key = key_vec * lax.rsqrt(jnp.sum(key_vec * key_vec, axis=-1, keepdims=True) + KEY_EPS)
    carried = state.reshape(seqs, heads, HEAD, HEAD).astype(F32)
    removed = jnp.sum(carried * unit_key[:, :, None, :], axis=-1)
    kept = jnp.sum(carried * (decay_rate * receptance)[:, :, None, :], axis=-1)
    steer = in_rate * receptance
    down_by = jnp.sum(unit_key * steer, axis=-1, keepdims=True)
    up_by = jnp.sum(key_vec * steer, axis=-1, keepdims=True)
    readout = kept - removed * down_by + value_vec * up_by
    centre = jnp.mean(readout, axis=-1, keepdims=True)
    spread = jnp.mean(jnp.square(readout - centre), axis=-1, keepdims=True)
    mixed = (readout - centre) * lax.rsqrt(spread + GN_EPS)
    return (mixed * head_gain).reshape(seqs, part).astype(BF16)


def attend_kernel(sizes, place, rows, *refs):
    z_size, x_size, tp = sizes
    lines, weights, out = refs[:z_size], refs[-2:-1] + refs[z_size:-2], refs[-1]
    z, x, core, shard = (place[index] for index in range(4))
    seqs, cols = lines[0].shape[0], weights[0].shape[1]
    z_tp = z_size // tp
    left = jnp.concatenate([line[...] for line in lines], axis=0)
    holds = (z // z_tp == shard).astype(F32)
    for step in range(x_size):
        weight = jnp.concatenate([ref[...] for ref in weights[2 * step : 2 * step + 2]], axis=1)
        product = dot(left, weight)
        for side in range(2):
            slot = paired(x, step, x_size) * 2 + (core ^ side)
            offset = pl.multiple_of(((z % z_tp) * 2 * x_size + slot) * cols, cols)
            for line in range(z_size):
                z_to = paired(z, line, z_size)
                token = rows[z_to * x_size + x, :, pl.ds(offset, cols)].astype(F32)
                vals = product[line * seqs : (line + 1) * seqs, side * cols : (side + 1) * cols]
                out[z_to, slot] = (vals + token * holds).astype(BF16)


def attend(kernels, place, rows, lines, weights, tp, x_size):
    z_size = len(lines)
    seqs, part = lines[0].shape
    cols = weights[0].shape[1]
    shape = (z_size, 2 * x_size, seqs, cols)
    if kernels:
        kernel = functools.partial(attend_kernel, (z_size, x_size, tp))
        out = jax.ShapeDtypeStruct(shape, BF16)
        return call(kernel, out, place, rows, *lines, *weights[1:], late=weights[:1])
    z, x, core, shard = (place[index] for index in range(4))
    z_tp = z_size // tp
    z_order = jnp.stack([paired(z, i, z_size) for i in range(z_size)])
    x_order = jnp.stack([paired(x, i // 2, x_size) * 2 + (core ^ (i % 2)) for i in range(2 * x_size)])
    left = jnp.take(jnp.stack(lines), z_order, axis=0).reshape(z_size * seqs, part)
    weight = jnp.take(jnp.stack(weights), jnp.argsort(x_order), axis=0)
    product = jnp.einsum("rk,skc->rsc", left, weight, preferred_element_type=F32)
    token = lax.dynamic_index_in_dim(
        rows.reshape(z_size, x_size, seqs, z_tp, 2 * x_size, cols), x, 1, keepdims=False
    )
    token = lax.dynamic_index_in_dim(token, z % z_tp, 2, keepdims=False).astype(F32)
    product = product.reshape(z_size, seqs, 2 * x_size, cols)
    product = product + jnp.where(z // z_tp == shard, token, 0.0)
    return product.astype(BF16).reshape(z_size, 1, seqs, 2 * x_size * cols)


def residual_kernel(place, tables, *refs):
    *parts, out = refs
    lines, slots, seqs, cols = parts[0].shape
    for line in range(lines):
        for slot in range(slots):
            vals = sum(part[line, slot].astype(F32) for part in parts).astype(BF16)
            out[line * slots + slot] = vals
    for index in range(tables.shape[0]):
        out[lines * slots + index] = tables[index]


def residual(kernels, place, parts, tables):
    lines, slots, seqs, cols = parts[0].shape
    tiles = lines * slots + tables.shape[0]
    if kernels:
        shape = jax.ShapeDtypeStruct((tiles, seqs, cols), BF16)
        return call(residual_kernel, shape, place, tables, *parts)
    total = sum(part.astype(F32) for part in parts).astype(BF16)
    return jnp.concatenate((total.reshape(lines * slots, seqs, cols), tables), axis=0)


def expert_kernel(sizes, place, *refs):
    x_size, experts = sizes
    *refs, left, got = refs
    chips = got.shape[0]
    chip = place[0] * x_size + place[1]
    for step in range(chips):
        got[paired(chip, step, chips)] = refs[step][...]
    gain, *refs = refs[chips:]
    own, other = (refs[0], refs[1], refs[4]), (refs[2], refs[3], refs[5])
    out, resid, home = refs[6:]
    chips, tp, seqs, part = out.shape
    z_size = chips // x_size
    cols = got.shape[3]
    slots = 2 * x_size
    width = part * tp
    count = chips * seqs
    z, x, core, shard = (place[index] for index in range(4))
    for index in range(chips):
        z_to, x_from = divmod(index, x_size)
        square = jnp.zeros((seqs, cols), F32)
        pieces = []
        for z_from in range(z_size):
            for slot in range(slots):
                piece = got[z_from * x_size + x_from, z_to * slots + slot].astype(F32)
                square = square + piece * piece
                pieces.append(piece)
        factor = lax.rsqrt(jnp.sum(square, axis=1, keepdims=True) / width + RMS_EPS)
        for block, piece in enumerate(pieces):
            lanes = slice(block * cols, (block + 1) * cols)
            left[index, :, lanes] = (piece * factor * gain[:, lanes]).astype(BF16)
    for z_part in range(z_size // tp):
        for slot in range(slots):
            block = z_part * slots + slot
            source = (shard * (z_size // tp) + z_part) * x_size + x
            resid[:, block * cols : (block + 1) * cols] = got[source, z * slots + slot]
    rows = left[...].reshape(count, width)
    tables = [
        got[:, z_size * slots + index].astype(F32).reshape(count, cols)
        for index in range(got.shape[1] - z_size * slots)
    ]
    tables = tables[0] if len(tables) == 1 else jnp.concatenate(tables, axis=1)
    lane = lax.broadcasted_iota(jnp.int32, tables.shape, 1)

    def hidden_of(vals, weights):
        gate, up, _ = weights
        return jax.nn.silu(dot(vals, gate[...])) * dot(vals, up[...])

    def scaled(weights, expert):
        hit = (lane == expert) | (lane == experts + expert)
        scale = jnp.sum(jnp.where(hit, tables, 0.0), axis=1, keepdims=True)
        return (hidden_of(rows, weights) * scale).astype(BF16)

    own_hidden = scaled(own, chip * 2 + core)
    other_hidden = scaled(other, chip * 2 + 1 - core)
    home[...] = left[chip]
    for target in range(tp):
        for start in range(0, part, 512):
            lanes = slice(start, min(start + 512, part))
            span = slice(target * part + lanes.start, target * part + lanes.stop)
            vals = dot(own_hidden, own[2][:, span]) + dot(other_hidden, other[2][:, span])
            vals = vals.reshape(chips, seqs, lanes.stop - lanes.start)
            out[:, target, :, lanes] = vals.astype(BF16)


def expert_rows(kernels, place, got, gain, own, other, tp, x_size):
    chips = len(got) if kernels else got.shape[0]
    seqs, cols = got[0].shape[-2:]
    z_size = chips // x_size
    width = gain.shape[1]
    slots = width // (z_size * cols)
    part = width // tp
    experts = 2 * chips
    if kernels:
        kernel = functools.partial(expert_kernel, (x_size, experts))
        shapes = [
            jax.ShapeDtypeStruct((chips, tp, seqs, part), BF16),
            jax.ShapeDtypeStruct((seqs, part), BF16),
            jax.ShapeDtypeStruct((seqs, width), BF16),
        ]
        scratch = (
            pltpu.VMEM((chips, seqs, width), BF16),
            pltpu.VMEM((chips,) + got[0].shape, BF16),
        )
        later = other[:2] + (own[2], other[2])
        return call(
            kernel, shapes, place, *got, gain, *own[:2], scratch=scratch, late=later
        )
    chip = place[0] * place[4] + place[1]
    rows = got[:, : z_size * slots].reshape(z_size, x_size, z_size, slots, seqs, cols)
    rows = rows.transpose(2, 1, 4, 0, 3, 5).reshape(chips, seqs, width)
    resid = lax.dynamic_index_in_dim(rows, chip, 0, keepdims=False)
    resid = lax.dynamic_slice_in_dim(resid, place[3] * part, part, 1)
    rows = rows.astype(F32)
    factor = lax.rsqrt(jnp.mean(rows * rows, axis=2, keepdims=True) + RMS_EPS)
    rows = (rows * factor * gain).astype(BF16)
    left = rows.reshape(chips * seqs, width)
    tables = got[:, z_size * slots :].astype(F32).transpose(0, 2, 1, 3).reshape(chips * seqs, -1)
    tables = tables[:, :experts] + tables[:, experts : 2 * experts]
    names = jnp.arange(experts, dtype=jnp.int32)[None, :]

    def hidden_of(vals, weights):
        gate, up, _ = weights
        return jax.nn.silu(dot(vals, gate)) * dot(vals, up)

    def product(weights, expert):
        scale = jnp.sum(jnp.where(names == expert, tables, 0.0), axis=1, keepdims=True)
        return dot((hidden_of(left, weights) * scale).astype(BF16), weights[2])

    routed = product(own, chip * 2 + place[2]) + product(other, chip * 2 + 1 - place[2])
    home = lax.dynamic_index_in_dim(rows, chip, 0, keepdims=False)
    routed = routed.astype(BF16).reshape(chips, seqs, tp, part).transpose(0, 2, 1, 3)
    return routed, resid, home


def shared_kernel(place, home, gate, up, down, *refs):
    *outs, whole = refs
    tp, seqs, part = whole.shape
    hidden = jax.nn.silu(dot(home[...], gate[...])) * dot(home[...], up[...])
    hidden = hidden.astype(BF16)
    for target in range(tp):
        whole[target] = dot(hidden, down[:, target * part : (target + 1) * part]).astype(BF16)
    for step, out in enumerate(outs):
        out[...] = whole[paired(place[3], step, tp)]


def shared_rows(kernels, place, home, weights, tp):
    seqs, width = home.shape
    part = width // tp
    if kernels:
        outs = [jax.ShapeDtypeStruct((seqs, part), BF16)] * tp
        scratch = (pltpu.VMEM((tp, seqs, part), BF16),)
        return call(shared_kernel, outs, place, home, *weights, scratch=scratch)
    gate, up, down = weights
    hidden = (jax.nn.silu(dot(home, gate)) * dot(home, up)).astype(BF16)
    whole = dot(hidden, down).astype(BF16)
    return [
        lax.dynamic_slice_in_dim(whole, paired(place[3], step, tp) * part, part, 1)
        for step in range(tp)
    ]


def body(
    tokens,
    state,
    mix_gain,
    w_recept,
    w_key,
    w_value,
    w_decay,
    w_rate,
    decay_base,
    rate_base,
    head_gain,
    w_out,
    moe_gain,
    routes,
    route_weight,
    expert_gate,
    expert_up,
    expert_down,
    shared_gate,
    shared_up,
    shared_down,
):
    z_size, x_size, tp = (lax.axis_size(name) for name in ("z", "x", "tp"))
    chips = z_size * x_size
    seqs, part = tokens.shape
    width = part * tp
    cols = w_out.shape[1]
    experts = 2 * chips
    kernels = cols == LANES and seqs == 16 and part % LANES == 0
    z, x, core, shard = (lax.axis_index(name) for name in ("z", "x", "core", "tp"))
    place = (z, x, core, shard, x_size)
    if kernels:
        place = jnp.stack([jnp.int32(index) for index in place])

    rows = spread_rows(tokens)
    own_w = (w_recept, w_key, w_value, w_decay, w_rate)
    other_w = tuple(swap_pairs(weight, "core", 1) for weight in own_w)
    mix_gain = mix_gain.reshape(1, part)
    moe_gain = moe_gain.reshape(1, width)
    blocks = (chips // tp, 2, 1, cols)
    decay_base, rate_base = decay_base.reshape(blocks), rate_base.reshape(blocks)
    head_gain = head_gain.reshape(part // HEAD, HEAD)
    if kernels:
        mix_gain, moe_gain, state = fetch(mix_gain, moe_gain, state)
    sent = project(kernels, place, rows, mix_gain, own_w, other_w)
    got = lax.all_to_all(sent, ("z", "x"), 0, 0, tiled=True)
    parts = pick(kernels, place, got, tokens, tp)
    parts = [swap_pairs(part_sum, "tp", index + 1) for index, part_sum in enumerate(parts)]
    mixed = mixer(
        kernels, place, got, tokens, state, parts, decay_base, rate_base, head_gain
    )

    out_w = []
    for step in range(x_size):
        weight = w_out if step == 0 else swap_pairs(w_out, "x", step)
        out_w += [weight, swap_pairs(weight, "core", 1)]
    lines = [mixed] + [swap_pairs(mixed, "z", step) for step in range(1, z_size)]
    partial = attend(kernels, place, rows, lines, out_w, tp, x_size)
    partials = [partial] + [swap_pairs(partial, "tp", step) for step in range(1, tp)]

    share = route_weight / jnp.sum(route_weight, axis=1, keepdims=True) * ROUTED_SCALE
    hit = routes[:, :, None] == jnp.arange(experts, dtype=jnp.int32)[None, None, :]
    table = jnp.sum(jnp.where(hit, share[:, :, None], 0.0), axis=1)
    high = table.astype(BF16)
    low = (table - high.astype(F32)).astype(BF16)
    lanes = partial.shape[3]
    pad = jnp.zeros((seqs, -(2 * experts) % lanes), BF16)
    tables = jnp.concatenate((high, low, pad), axis=1)
    tables = tables.reshape(seqs, -1, lanes).transpose(1, 0, 2)
    packed = residual(kernels, place, partials, tables)
    if kernels:
        got = [packed] + [swap_chips(packed, step, chips) for step in range(1, chips)]
    else:
        got = spread_rows(packed)

    own = (expert_gate[0], expert_up[0], expert_down[0])
    other = tuple(swap_pairs(weight, "core", 1) for weight in own)
    routed, resid, home = expert_rows(kernels, place, got, moe_gain, own, other, tp, x_size)
    routed = routed.reshape(chips * tp, seqs, part)
    returned = lax.all_to_all(routed, ("z", "x", "tp"), 0, 0, tiled=True)
    added = shared_rows(kernels, place, home, (shared_gate, shared_up, shared_down), tp)
    added = [added[0]] + [swap_pairs(added[step], "tp", step) for step in range(1, tp)]
    total = resid.astype(F32) + sum(piece.astype(F32) for piece in added)
    return (total + jnp.sum(returned.astype(F32), axis=0)).astype(BF16)


def solution(mesh):
    ep, tp = mesh.shape["ep"], mesh.shape["tp"]
    lines = mesh.devices.reshape(ep // 2, 2, tp)
    x_size = len({getattr(device, "coords", (0,))[0] for device in lines[:, 0, 0]})
    grid = Mesh(lines.reshape(-1, x_size, 2, tp), ("z", "x", "core", "tp"))
    ep = ("z", "x", "core")
    placed = (
        P(ep, "tp"),
        P(ep, "tp", None),
        P("tp"),
        P("tp", ep),
        P("tp", ep),
        P("tp", ep),
        P("tp", ep),
        P("tp", ep),
        P("tp"),
        P("tp"),
        P("tp"),
        P("tp", ep),
        P(),
        P(ep, None),
        P(ep, None),
        P(ep, None, "tp"),
        P(ep, None, "tp"),
        P(ep, "tp", None),
        P(None, "tp"),
        P(None, "tp"),
        P("tp", None),
    )
    return jax.shard_map(body, mesh=grid, in_specs=placed, out_specs=P(ep, "tp"), check_vma=False)
```

```python
import functools

import jax
import jax.numpy as jnp
from jax import lax
from jax.experimental import pallas as pl
from jax.experimental.pallas import tpu as pltpu
from jax.sharding import Mesh, PartitionSpec as P


HEAD = 64
LANES = 128


RMS_EPS = 1e-06
GN_EPS = 0.00064
KEY_EPS = 1e-06
ROUTED_SCALE = 2.5

F32 = jnp.float32
BF16 = jnp.bfloat16


def dot(left, right):
    return jnp.dot(left, right, preferred_element_type=F32)


def paired(index, step, count):
    if count & (count - 1) == 0:
        return index ^ step
    return (step - index) % count


def swap_pairs(array, axis, step):
    count = lax.axis_size(axis)
    return lax.ppermute(array, axis, [(i, paired(i, step, count)) for i in range(count)])


def spread_pieces(piece):
    lines = [piece] + [swap_pairs(piece, "z", step) for step in range(1, lax.axis_size("z"))]
    pieces = []
    for line in lines:
        pieces += [line] + [swap_pairs(line, "x", step) for step in range(1, lax.axis_size("x"))]
    return pieces


def spread_rows(rows):
    copies = jnp.broadcast_to(rows[None], (lax.axis_size("z") * lax.axis_size("x"),) + rows.shape)
    return lax.all_to_all(copies, ("z", "x"), 0, 0, tiled=True)


class Late:
    def __init__(self, source, held, arrival):
        self.held, self.shape = held, held.shape
        self.copy = pltpu.make_async_copy(source, held, arrival)
        self.copy.start()
        self.waited = False

    def __getitem__(self, index):
        if not self.waited:
            self.copy.wait()
            self.waited = True
        return self.held[index]


def call(kernel, outs, place, *operands, scratch=(), late=()):
    hbm, vmem = (pl.BlockSpec(memory_space=space) for space in (pltpu.HBM, pltpu.VMEM))
    single = not isinstance(outs, list)
    outs = [outs] if single else outs
    counts = len(operands), len(late), len(outs), len(scratch)
    operands = [pltpu.with_memory_space_constraint(array, pltpu.VMEM) for array in operands]
    later = [pltpu.with_memory_space_constraint(array, pltpu.HBM) for array in late]
    buffers = [pltpu.VMEM(array.shape, array.dtype) for array in late]
    if late:
        buffers.append(pltpu.SemaphoreType.DMA((len(late),)))

    def with_copies(place, *refs):
        parts = []
        for count in counts:
            parts.append(refs[:count])
            refs = refs[count:]
        given, sources, results, own = parts
        waiting = [
            Late(source, held, refs[-1].at[index])
            for index, (source, held) in enumerate(zip(sources, refs))
        ]
        kernel(place, *given, *waiting, *results, *own)

    results = pl.pallas_call(
        with_copies,
        out_shape=outs,
        in_specs=[pl.BlockSpec(memory_space=pltpu.SMEM)]
        + [vmem] * len(operands)
        + [hbm] * len(later),
        out_specs=[vmem] * len(outs),
        scratch_shapes=list(scratch) + buffers,
        compiler_params=pltpu.CompilerParams(vmem_limit_bytes=24 * 1024 * 1024),
    )(place, *operands, *later)
    return results[0] if single else results


def fetch_kernel(array, after, held, arrival):
    copy = pltpu.make_async_copy(array, held, arrival)
    copy.start()
    copy.wait()


def fetch(array, after):
    hbm, vmem = pltpu.HBM, pltpu.VMEM
    return pl.pallas_call(
        fetch_kernel,
        out_shape=pltpu.VMEM(array.shape, array.dtype),
        in_specs=[pl.BlockSpec(memory_space=hbm), pl.BlockSpec(memory_space=vmem)],
        out_specs=pl.BlockSpec(memory_space=vmem),
        scratch_shapes=[pltpu.SemaphoreType.DMA(())],
        compiler_params=pltpu.CompilerParams(vmem_limit_bytes=24 * 1024 * 1024),
    )(
        pltpu.with_memory_space_constraint(array, hbm),
        pltpu.with_memory_space_constraint(after, vmem),
    )


def project_kernel(sizes, place, *refs):
    chips, roles, x_size, tp = sizes
    other, given, refs = refs[:roles], refs[roles : roles + chips], refs[roles + chips :]
    gain, own = refs[0], refs[1 : roles + 1]
    out, kept, rows = refs[roles + 1 :]
    core = place[2]
    chip = place[0] * place[4] + place[1]
    for step in range(chips):
        rows[paired(chip, step, chips)] = given[step][...]
    chips, seqs, part = rows.shape
    cols = own[0].shape[1]
    z_size, slots = kept.shape[:2]
    z_tp = z_size // tp
    holds = (place[0] // z_tp == place[3]).astype(F32)
    for line in range(z_size):
        for slot in range(slots):
            offset = pl.multiple_of((place[0] % z_tp * slots + slot) * cols, cols)
            vals = rows[line * x_size + place[1], :, pl.ds(offset, cols)].astype(F32) * holds
            kept[line, slot] = vals.astype(BF16)
    scaled = (rows[...].astype(F32) * gain[...]).reshape(chips * seqs, part).astype(BF16)
    order = [(role, 1 - core, other[role]) for role in range(roles)]
    order += [(role, core, own[role]) for role in range(roles)]
    for first in range(0, 2 * roles, 2):
        pair = order[first : first + 2]
        weight = jnp.concatenate([ref[...] for _, _, ref in pair], axis=1)
        product = dot(scaled, weight).astype(BF16).reshape(chips, seqs, 2 * cols)
        for index, (role, side, _) in enumerate(pair):
            out[:, role, side] = product[:, :, index * cols : (index + 1) * cols]


def project(kernels, place, rows, gain, own, other, tp, x_size):
    chips = len(rows) if kernels else rows.shape[0]
    seqs, part = rows[0].shape
    cols = own[0].shape[1]
    roles = len(own)
    if kernels:
        kernel = functools.partial(project_kernel, (chips, roles, x_size, tp))
        outs = [
            jax.ShapeDtypeStruct((chips, roles, 2, seqs, cols), BF16),
            pltpu.VMEM((chips // x_size, 2 * x_size, seqs, cols), BF16),
        ]
        scratch = (pltpu.VMEM((chips, seqs, part), BF16),)
        later = tuple(rows) + (gain,) + own
        return call(kernel, outs, place, *other, scratch=scratch, late=later)
    scaled = (rows.astype(F32) * gain[0]).astype(BF16).reshape(chips * seqs, part)
    pairs = []
    for mine, theirs in zip(own, other):
        sides = jnp.stack((dot(scaled, mine), dot(scaled, theirs))).astype(BF16)
        pairs.append(jnp.where(place[2] == 0, sides, sides[::-1]))
    product = jnp.stack(pairs).reshape(roles, 2, chips, seqs, cols)
    z, x, shard = place[0], place[1], place[3]
    z_size = chips // x_size
    z_tp = z_size // tp
    kept = rows.reshape(z_size, x_size, seqs, z_tp, 2 * x_size * cols)
    kept = lax.dynamic_index_in_dim(kept, x, 1, keepdims=False)
    kept = lax.dynamic_index_in_dim(kept, z % z_tp, 2, keepdims=False)
    kept = jnp.where(z // z_tp == shard, kept, jnp.zeros_like(kept))
    return product.transpose(2, 0, 1, 3, 4), kept


def square_of(tokens):
    vals = tokens.astype(F32)
    return jnp.sum(vals * vals, axis=1, keepdims=True)


def pick_kernel(place, got, tokens, *outs):
    chips, roles, sides, seqs, cols = got.shape
    chips_tp = chips // (len(outs) + 1)
    count = chips_tp * roles * sides
    square = square_of(tokens[...])
    high = square.astype(BF16).astype(F32)
    for step, out in enumerate(outs):
        target = paired(place[3], step + 1, len(outs) + 1)
        block = got[pl.ds(target * chips_tp, chips_tp)]
        out[:count] = block.reshape(count, seqs, cols)
        out[count] = jnp.broadcast_to(high, (seqs, cols)).astype(BF16)
        out[count + 1] = jnp.broadcast_to(square - high, (seqs, cols)).astype(BF16)


def pick(kernels, place, got, tokens, tp):
    chips, roles, sides, seqs, cols = got.shape
    chips_tp = chips // tp
    count = chips_tp * roles * sides
    if kernels:
        outs = [pltpu.VMEM((count + 2, seqs, cols), BF16)] * (tp - 1)
        return call(pick_kernel, outs, place, got, tokens)
    square = square_of(tokens)
    high = square.astype(BF16)
    marks = jnp.stack((high, (square - high.astype(F32)).astype(BF16)))
    marks = jnp.broadcast_to(marks, (2, seqs, cols))
    outs = []
    for step in range(1, tp):
        start = paired(place[3], step, tp) * chips_tp
        block = lax.dynamic_slice_in_dim(got, start, chips_tp, 0)
        outs.append(jnp.concatenate((block.reshape(count, seqs, cols), marks), axis=0))
    return outs


def gates(decay_pre, rate_pre):
    decay_rate = jnp.exp(-jnp.exp(-jax.nn.softplus(-decay_pre) - 0.5))
    return decay_rate, jax.nn.sigmoid(rate_pre)


def mixer_kernel(place, got, tokens, state, *refs):
    *parts, bases, out, products, flat = refs
    chips, roles, sides, seqs, cols = got.shape
    tp = len(parts) + 1
    chips_tp = chips // tp
    heads = state.shape[1]
    count = seqs * heads
    half = count // 2
    blocks = chips_tp * roles * sides
    square = square_of(tokens[...])
    for part in parts:
        square = square + part[blocks].astype(F32) + part[blocks + 1].astype(F32)
    factor = lax.rsqrt(square / (heads * HEAD * tp) + RMS_EPS)
    others = [part[:blocks].reshape(chips_tp, roles, sides, seqs, cols) for part in parts]

    def role(index, base=None):
        vals = got[pl.ds(place[3] * chips_tp, chips_tp), index].astype(F32)
        for other in others:
            vals = vals + other[:, index].astype(F32)
        vals = vals * factor
        if base is not None:
            vals = vals + bases[base]
        return vals.reshape(half, LANES)

    receptance, key_vec, value_vec = role(0), role(1), role(2)
    row = lax.broadcasted_iota(jnp.int32, (LANES, LANES), 0)
    lane = lax.broadcasted_iota(jnp.int32, (LANES, LANES), 1)
    same_head = (row // HEAD == lane // HEAD).astype(F32)

    def head_sum(vals):
        return jnp.dot(
            vals, same_head, precision=lax.Precision.HIGHEST, preferred_element_type=F32
        )

    unit_key = key_vec * lax.rsqrt(head_sum(key_vec * key_vec) + KEY_EPS)
    decay_rate, in_rate = gates(role(3, 0), role(4, 1))
    steer = in_rate * receptance
    down_by = head_sum(unit_key * steer)
    raised = value_vec * head_sum(key_vec * steer)
    side = lax.broadcasted_iota(jnp.int32, (half, LANES), 1) < HEAD
    evens, odds = [], []
    for vals in (decay_rate * receptance, unit_key, raised, down_by):
        turned = pltpu.roll(vals, HEAD, 1)
        evens.append(jnp.where(side, vals, turned))
        odds.append(jnp.where(side, turned, vals))
    stacked = jnp.concatenate(
        (jnp.concatenate(evens, axis=1), jnp.concatenate(odds, axis=1)), axis=0
    )
    high = stacked.astype(BF16)
    low = (stacked - high.astype(F32)).astype(BF16)
    row = lax.broadcasted_iota(jnp.int32, (count, count), 0)
    col = lax.broadcasted_iota(jnp.int32, (count, count), 1)
    block = (col % half) // seqs
    chosen = (row // heads == col % seqs) & (row % heads == 2 * block + col // half)
    chosen = chosen.astype(F32).astype(BF16)
    turned = dot(chosen, high) + dot(chosen, low)
    along, unit, raised, down_by = (
        turned[:, index * LANES : (index + 1) * LANES] for index in range(4)
    )
    along = jnp.concatenate((along, along), axis=1)
    unit = jnp.concatenate((unit, unit), axis=1)
    span = 2 * LANES
    for start in range(0, HEAD * HEAD, span):
        vals = state[:, :, start : start + span].reshape(count, span).astype(F32)
        products[:count, start : start + span] = (vals * along).astype(BF16)
        products[count:, start : start + span] = (vals * unit).astype(BF16)
    row = lax.broadcasted_iota(jnp.int32, (HEAD * HEAD, HEAD), 0)
    col = lax.broadcasted_iota(jnp.int32, (HEAD * HEAD, HEAD), 1)
    sums = dot(products[...], (row // HEAD == col).astype(F32).astype(BF16))
    readout = sums[:count] - sums[count:] * down_by[:, :HEAD] + raised[:, :HEAD]
    readout = readout - jnp.mean(readout, axis=-1, keepdims=True)
    spread = jnp.mean(readout * readout, axis=-1, keepdims=True)
    normed = readout * lax.rsqrt(spread + GN_EPS)
    flat[...] = normed
    for index in range(0, heads, 2):
        first = flat[pl.ds(index, seqs, stride=heads), :]
        second = flat[pl.ds(index + 1, seqs, stride=heads), :]
        vals = jnp.concatenate((first, second), axis=1)
        vals = vals * bases[2, index // (2 * sides), index // 2 % sides]
        out[:, index * HEAD : (index + 2) * HEAD] = vals.astype(BF16)


def mixer(kernels, place, got, tokens, state, parts, bases):
    seqs, heads, _ = state.shape
    chips, roles, sides, _, cols = got.shape
    tp = len(parts) + 1
    chips_tp = chips // tp
    part = heads * HEAD
    if kernels:
        return call(
            mixer_kernel,
            pltpu.VMEM((seqs, part), BF16),
            place,
            got,
            tokens,
            state,
            *parts,
            bases,
            scratch=(
                pltpu.VMEM((2 * seqs * heads, HEAD * HEAD), BF16),
                pltpu.VMEM((seqs * heads, HEAD), F32),
            ),
        )
    square = square_of(tokens) + sum(other[-2:].astype(F32).sum(0)[:, :1] for other in parts)
    factor = lax.rsqrt(square / (part * tp) + RMS_EPS)
    total = lax.dynamic_slice_in_dim(got, place[3] * chips_tp, chips_tp, 0).astype(F32)
    for other in parts:
        total = total + other[:-2].astype(F32).reshape(total.shape)
    total = total * factor
    total = total.transpose(1, 3, 0, 2, 4).reshape(roles, seqs, part)

    def per_head(vals):
        return vals.reshape(-1, heads, HEAD)

    receptance, key_vec, value_vec = (per_head(total[i]) for i in range(3))
    decay_rate, in_rate = gates(
        per_head(total[3]) + per_head(bases[0]), per_head(total[4]) + per_head(bases[1])
    )
    unit_key = key_vec * lax.rsqrt(jnp.sum(key_vec * key_vec, axis=-1, keepdims=True) + KEY_EPS)
    carried = state.reshape(seqs, heads, HEAD, HEAD).astype(F32)
    removed = jnp.sum(carried * unit_key[:, :, None, :], axis=-1)
    kept = jnp.sum(carried * (decay_rate * receptance)[:, :, None, :], axis=-1)
    steer = in_rate * receptance
    down_by = jnp.sum(unit_key * steer, axis=-1, keepdims=True)
    up_by = jnp.sum(key_vec * steer, axis=-1, keepdims=True)
    readout = kept - removed * down_by + value_vec * up_by
    centre = jnp.mean(readout, axis=-1, keepdims=True)
    spread = jnp.mean(jnp.square(readout - centre), axis=-1, keepdims=True)
    mixed = (readout - centre) * lax.rsqrt(spread + GN_EPS)
    return (mixed * per_head(bases[2])).reshape(seqs, part).astype(BF16)


def attend_kernel(sizes, place, kept, *refs):
    z_size, x_size = sizes
    lines, weights, out = refs[:z_size], refs[-2:-1] + refs[z_size:-2], refs[-1]
    z, x, core = (place[index] for index in range(3))
    seqs, cols = lines[0].shape[0], weights[0].shape[1]
    left = jnp.concatenate([line[...] for line in lines], axis=0)
    for step in reversed(range(x_size)):
        weight = jnp.concatenate([ref[...] for ref in weights[2 * step : 2 * step + 2]], axis=1)
        product = dot(left, weight)
        for side in range(2):
            slot = paired(x, step, x_size) * 2 + (core ^ side)
            for line in range(z_size):
                z_to = paired(z, line, z_size)
                vals = product[line * seqs : (line + 1) * seqs, side * cols : (side + 1) * cols]
                out[z_to, slot] = (vals + kept[z_to, slot].astype(F32)).astype(BF16)


def attend(kernels, place, kept, lines, weights, x_size):
    z_size = len(lines)
    seqs, part = lines[0].shape
    cols = weights[0].shape[1]
    if kernels:
        kernel = functools.partial(attend_kernel, (z_size, x_size))
        out = pltpu.VMEM((z_size, 2 * x_size, seqs, cols), BF16)
        return call(kernel, out, place, kept, *lines, *weights[1:], late=weights[:1])
    z, x, core = (place[index] for index in range(3))
    z_order = jnp.stack([paired(z, i, z_size) for i in range(z_size)])
    x_order = jnp.stack([paired(x, i // 2, x_size) * 2 + (core ^ (i % 2)) for i in range(2 * x_size)])
    left = jnp.take(jnp.stack(lines), z_order, axis=0).reshape(z_size * seqs, part)
    weight = jnp.take(jnp.stack(weights), jnp.argsort(x_order), axis=0)
    product = jnp.einsum("rk,skc->rsc", left, weight, preferred_element_type=F32)
    product = product.reshape(z_size, seqs, 2 * x_size * cols) + kept.astype(F32)
    return product.astype(BF16)[:, None]


def residual_kernel(place, tables, *refs):
    *parts, out = refs
    lines, slots, seqs, cols = parts[0].shape
    for line in range(lines):
        for slot in range(slots):
            vals = sum(part[line, slot].astype(F32) for part in parts).astype(BF16)
            out[line * slots + slot] = vals
    for index in range(tables.shape[0]):
        out[lines * slots + index] = tables[index]


def residual(kernels, place, parts, tables):
    lines, slots, seqs, cols = parts[0].shape
    tiles = lines * slots + tables.shape[0]
    if kernels:
        shape = pltpu.VMEM((tiles, seqs, cols), BF16)
        return call(residual_kernel, shape, place, tables, *parts)
    total = sum(part.astype(F32) for part in parts).astype(BF16)
    return jnp.concatenate((total.reshape(lines * slots, seqs, cols), tables), axis=0)


def expert_kernel(sizes, place, *refs):
    x_size, experts = sizes
    *refs, left, got = refs
    chips = got.shape[0]
    chip = place[0] * x_size + place[1]
    for step in range(chips):
        got[paired(chip, step, chips)] = refs[step][...]
    refs = refs[chips:]
    own, other, gain = (refs[0], refs[1], refs[5]), (refs[3], refs[4], refs[6]), refs[2]
    out, resid, home = refs[7:]
    chips, tp, seqs, part = out.shape
    z_size = chips // x_size
    cols = got.shape[3]
    slots = 2 * x_size
    width = part * tp
    count = chips * seqs
    z, x, core, shard = (place[index] for index in range(4))
    for index in range(chips):
        z_to, x_from = divmod(index, x_size)
        square = jnp.zeros((seqs, cols), F32)
        pieces = []
        for z_from in range(z_size):
            for slot in range(slots):
                piece = got[z_from * x_size + x_from, z_to * slots + slot].astype(F32)
                square = square + piece * piece
                pieces.append(piece)
        factor = lax.rsqrt(jnp.sum(square, axis=1, keepdims=True) / width + RMS_EPS)
        for block, piece in enumerate(pieces):
            lanes = slice(block * cols, (block + 1) * cols)
            left[index, :, lanes] = (piece * factor * gain[:, lanes]).astype(BF16)
    for z_part in range(z_size // tp):
        for slot in range(slots):
            block = z_part * slots + slot
            source = (shard * (z_size // tp) + z_part) * x_size + x
            resid[:, block * cols : (block + 1) * cols] = got[source, z * slots + slot]
    rows = left[...].reshape(count, width)
    tables = [
        got[:, z_size * slots + index].astype(F32).reshape(count, cols)
        for index in range(got.shape[1] - z_size * slots)
    ]
    tables = tables[0] if len(tables) == 1 else jnp.concatenate(tables, axis=1)
    lane = lax.broadcasted_iota(jnp.int32, tables.shape, 1)

    def hidden_of(vals, weights):
        gate, up, _ = weights
        return jax.nn.silu(dot(vals, gate[...])) * dot(vals, up[...])

    def scaled(weights, expert):
        hit = (lane == expert) | (lane == experts + expert)
        scale = jnp.sum(jnp.where(hit, tables, 0.0), axis=1, keepdims=True)
        return (hidden_of(rows, weights) * scale).astype(BF16)

    own_hidden = scaled(own, chip * 2 + core)
    other_hidden = scaled(other, chip * 2 + 1 - core)
    home[...] = left[chip]
    for target in range(tp):
        for start in range(0, part, 512):
            lanes = slice(start, min(start + 512, part))
            span = slice(target * part + lanes.start, target * part + lanes.stop)
            vals = dot(own_hidden, own[2][:, span]) + dot(other_hidden, other[2][:, span])
            vals = vals.reshape(chips, seqs, lanes.stop - lanes.start)
            out[:, target, :, lanes] = vals.astype(BF16)


def expert_rows(kernels, place, got, gain, own, other, tp, x_size):
    chips = len(got) if kernels else got.shape[0]
    seqs, cols = got[0].shape[-2:]
    z_size = chips // x_size
    width = gain.shape[1]
    slots = width // (z_size * cols)
    part = width // tp
    experts = 2 * chips
    if kernels:
        kernel = functools.partial(expert_kernel, (x_size, experts))
        shapes = [
            jax.ShapeDtypeStruct((chips, tp, seqs, part), BF16),
            pltpu.VMEM((seqs, part), BF16),
            pltpu.VMEM((seqs, width), BF16),
        ]
        scratch = (
            pltpu.VMEM((chips, seqs, width), BF16),
            pltpu.VMEM((chips,) + got[0].shape, BF16),
        )
        later = (gain,) + other[:2] + (own[2], other[2])
        return call(
            kernel, shapes, place, *got, *own[:2], scratch=scratch, late=later
        )
    chip = place[0] * place[4] + place[1]
    rows = got[:, : z_size * slots].reshape(z_size, x_size, z_size, slots, seqs, cols)
    rows = rows.transpose(2, 1, 4, 0, 3, 5).reshape(chips, seqs, width)
    resid = lax.dynamic_index_in_dim(rows, chip, 0, keepdims=False)
    resid = lax.dynamic_slice_in_dim(resid, place[3] * part, part, 1)
    rows = rows.astype(F32)
    factor = lax.rsqrt(jnp.mean(rows * rows, axis=2, keepdims=True) + RMS_EPS)
    rows = (rows * factor * gain[0]).astype(BF16)
    left = rows.reshape(chips * seqs, width)
    tables = got[:, z_size * slots :].astype(F32).transpose(0, 2, 1, 3).reshape(chips * seqs, -1)
    tables = tables[:, :experts] + tables[:, experts : 2 * experts]
    names = jnp.arange(experts, dtype=jnp.int32)[None, :]

    def hidden_of(vals, weights):
        gate, up, _ = weights
        return jax.nn.silu(dot(vals, gate)) * dot(vals, up)

    def product(weights, expert):
        scale = jnp.sum(jnp.where(names == expert, tables, 0.0), axis=1, keepdims=True)
        return dot((hidden_of(left, weights) * scale).astype(BF16), weights[2])

    routed = product(own, chip * 2 + place[2]) + product(other, chip * 2 + 1 - place[2])
    home = lax.dynamic_index_in_dim(rows, chip, 0, keepdims=False)
    routed = routed.astype(BF16).reshape(chips, seqs, tp, part).transpose(0, 2, 1, 3)
    return routed, resid, home


def shared_kernel(place, home, gate, up, down, *refs):
    *outs, whole = refs
    tp, seqs, part = whole.shape
    hidden = jax.nn.silu(dot(home[...], gate[...])) * dot(home[...], up[...])
    hidden = hidden.astype(BF16)
    for target in range(tp):
        whole[target] = dot(hidden, down[:, target * part : (target + 1) * part]).astype(BF16)
    for step, out in enumerate(outs):
        out[...] = whole[paired(place[3], step, tp)]


def shared_rows(kernels, place, home, weights, tp):
    seqs, width = home.shape
    part = width // tp
    if kernels:
        outs = [pltpu.VMEM((seqs, part), BF16)] * tp
        scratch = (pltpu.VMEM((tp, seqs, part), BF16),)
        return call(shared_kernel, outs, place, home, *weights, scratch=scratch)
    gate, up, down = weights
    hidden = (jax.nn.silu(dot(home, gate)) * dot(home, up)).astype(BF16)
    whole = dot(hidden, down).astype(BF16)
    return [
        lax.dynamic_slice_in_dim(whole, paired(place[3], step, tp) * part, part, 1)
        for step in range(tp)
    ]


def sum_kernel(place, returned, *refs):
    *pieces, out = refs
    total = sum(piece[...].astype(F32) for piece in pieces)
    for source in range(returned.shape[0]):
        total = total + returned[source].astype(F32)
    out[...] = total.astype(BF16)


def gather_up(kernels, place, returned, *pieces):
    if kernels:
        shape = jax.ShapeDtypeStruct(pieces[0].shape, BF16)
        return call(sum_kernel, shape, place, returned, *pieces)
    total = sum(piece.astype(F32) for piece in pieces)
    return (total + jnp.sum(returned.astype(F32), axis=0)).astype(BF16)


def body(
    tokens,
    state,
    mix_gain,
    w_recept,
    w_key,
    w_value,
    w_decay,
    w_rate,
    decay_base,
    rate_base,
    head_gain,
    w_out,
    moe_gain,
    routes,
    route_weight,
    expert_gate,
    expert_up,
    expert_down,
    shared_gate,
    shared_up,
    shared_down,
):
    z_size, x_size, tp = (lax.axis_size(name) for name in ("z", "x", "tp"))
    chips = z_size * x_size
    seqs, part = tokens.shape
    width = part * tp
    cols = w_out.shape[1]
    experts = 2 * chips
    kernels = cols == LANES and seqs == 16 and chips & (chips - 1) == 0
    z, x, core, shard = (lax.axis_index(name) for name in ("z", "x", "core", "tp"))
    place = (z, x, core, shard, x_size)
    if kernels:
        place = jnp.stack([jnp.int32(index) for index in place])

    rows = spread_pieces(tokens) if kernels else spread_rows(tokens)
    own_w = (w_recept, w_key, w_value, w_decay, w_rate)
    other_w = tuple(swap_pairs(weight, "core", 1) for weight in own_w)
    mix_gain = mix_gain.reshape(1, part)
    moe_gain = moe_gain.reshape(1, width)
    bases = jnp.stack((decay_base, rate_base, head_gain))
    bases = bases.reshape(3, chips // tp, 2, 1, cols)
    sent, kept = project(kernels, place, rows, mix_gain, own_w, other_w, tp, x_size)
    if kernels:
        state = fetch(state, kept)
    got = lax.all_to_all(sent, ("z", "x"), 0, 0, tiled=True)
    parts = pick(kernels, place, got, tokens, tp)
    parts = [swap_pairs(part_sum, "tp", index + 1) for index, part_sum in enumerate(parts)]
    mixed = mixer(kernels, place, got, tokens, state, parts, bases)

    out_w = []
    for step in range(x_size):
        weight = w_out if step == 0 else swap_pairs(w_out, "x", step)
        out_w += [weight, swap_pairs(weight, "core", 1)]
    lines = [mixed] + [swap_pairs(mixed, "z", step) for step in range(1, z_size)]
    partial = attend(kernels, place, kept, lines, out_w, x_size)
    partials = [partial] + [swap_pairs(partial, "tp", step) for step in range(1, tp)]

    share = route_weight / jnp.sum(route_weight, axis=1, keepdims=True) * ROUTED_SCALE
    hit = routes[:, :, None] == jnp.arange(experts, dtype=jnp.int32)[None, None, :]
    table = jnp.sum(jnp.where(hit, share[:, :, None], 0.0), axis=1)
    high = table.astype(BF16)
    low = (table - high.astype(F32)).astype(BF16)
    lanes = partial.shape[3]
    pad = jnp.zeros((seqs, -(2 * experts) % lanes), BF16)
    tables = jnp.concatenate((high, low, pad), axis=1)
    tables = tables.reshape(seqs, -1, lanes).transpose(1, 0, 2)
    packed = residual(kernels, place, partials, tables)
    if kernels:
        got = spread_pieces(packed)
    else:
        got = spread_rows(packed)

    own = (expert_gate[0], expert_up[0], expert_down[0])
    other = tuple(swap_pairs(weight, "core", 1) for weight in own)
    routed, resid, home = expert_rows(kernels, place, got, moe_gain, own, other, tp, x_size)
    routed = routed.reshape(chips * tp, seqs, part)
    returned = lax.all_to_all(routed, ("z", "x", "tp"), 0, 0, tiled=True)
    added = shared_rows(kernels, place, home, (shared_gate, shared_up, shared_down), tp)
    added = [added[0]] + [swap_pairs(added[step], "tp", step) for step in range(1, tp)]
    return gather_up(kernels, place, returned, resid, *added)


def solution(mesh):
    ep, tp = mesh.shape["ep"], mesh.shape["tp"]
    lines = mesh.devices.reshape(ep // 2, 2, tp)
    x_size = len({getattr(device, "coords", (0,))[0] for device in lines[:, 0, 0]})
    grid = Mesh(lines.reshape(-1, x_size, 2, tp), ("z", "x", "core", "tp"))
    ep = ("z", "x", "core")
    placed = (
        P(ep, "tp"),
        P(ep, "tp", None),
        P("tp"),
        P("tp", ep),
        P("tp", ep),
        P("tp", ep),
        P("tp", ep),
        P("tp", ep),
        P("tp"),
        P("tp"),
        P("tp"),
        P("tp", ep),
        P(),
        P(ep, None),
        P(ep, None),
        P(ep, None, "tp"),
        P(ep, None, "tp"),
        P(ep, "tp", None),
        P(None, "tp"),
        P(None, "tp"),
        P("tp", None),
    )
    return jax.shard_map(body, mesh=grid, in_specs=placed, out_specs=P(ep, "tp"), check_vma=False)
```
